256 devices in a mesh: fs: 32 (over z, y), tp: 8 (over x, core).
Axes of the slice: x: 4, y: 4, z: 8, core: 2. Of those that a mesh axis runs over, the one named last changes fastest.
Arguments:
- normed_input: bfloat16 [16384, 2048], P('fs', 'tp'), may hold values from -6 to 6
- cotangent: bfloat16 [16384, 2048], P('fs', 'tp'), may hold values from -6 to 6
- up_weight: bfloat16 [2048, 8192], P('fs', 'tp'), may hold values from -0.125 to 0.125
- down_weight: bfloat16 [8192, 2048], P('tp', 'fs'), may hold values from -0.0625 to 0.0625
Outputs:
- input_grad: bfloat16 [16384, 2048], P('fs', 'tp')
- up_grad: float32 [2048, 8192], P('fs', 'tp')
- down_grad: float32 [8192, 2048], P('tp', 'fs')
The draws below stay inside these ranges and needn't reach their ends.
All inputs are finite; a program needn't handle non-finite values.
Results may differ from the reference program's by a relative error of at most 0.018.
Values may be sent and summed in bfloat16 or wider, within the bound.
A program may use at most 64 MiB of HBM per device.

```python
import jax
import jax.numpy as jnp
from jax import lax

D = 2048
FF = 8192
TOKENS = 16384
FF_BLOCKS = 8


def strengthened(array, key, source, target, blocks, factor):
    owner, partner = [(jnp.arange(array.shape[axis_at]) // (array.shape[axis_at] // blocks)).reshape([-1 if axis == axis_at else 1 for axis in range(array.ndim)]) for axis_at in (source, target)]
    chosen = jax.random.permutation(key, blocks)[partner]
    strong = (owner == chosen) | (owner == (partner + blocks // 2) % blocks)
    return jnp.where(strong, factor * array, array)


def steps_of(stream_key, extent, shards, smallest, top_value):
    gain = 1.0
    for position, shards_of in shards:
        steps = jax.random.uniform(jax.random.fold_in(jax.random.fold_in(stream_key, 6), position), (shards_of,), jnp.float32, smallest / len(shards), top_value / len(shards))
        gain = gain * jnp.repeat(jnp.exp(steps), extent[position] // shards_of).reshape((-1,) + (1,) * (len(extent) - 1 - position))
    return gain


def bell_draw(stream_key, dims, spread, limit, pieces=(), kind=jnp.bfloat16):
    array = spread * jax.random.normal(stream_key, dims, jnp.float32)
    if pieces:
        array = array * steps_of(stream_key, dims, pieces, -0.22, 0.18)
    return jnp.clip(array, -limit, limit).astype(kind)


def heavy_noise(own_key, extent, spread, limit, cuts, heavy, kind=jnp.bfloat16):
    result = spread * jax.random.normal(own_key, extent, jnp.float32)
    if cuts:
        result = result * steps_of(own_key, extent, cuts, -0.22, 0.18)
    return jnp.clip(strengthened(result, jax.random.fold_in(own_key, 3), *heavy), -limit, limit).astype(kind)


def setup_inputs(seed: int = 0) -> dict:
    splits = jax.random.split(jax.random.key(seed), 5)
    normed_input = heavy_noise(splits[0], (TOKENS, D), 1.0, 6.0, ((0, 32), (1, 8)), (0, 1, 32, 2.75))
    cotangent = heavy_noise(splits[1], (TOKENS, D), 1.0, 6.0, ((0, 32), (1, 8)), (0, 1, 32, 2.75))
    up_weight = bell_draw(splits[2], (D, FF), D ** -0.5, 0.125, ((0, 32), (1, 8)))
    down_weight = bell_draw(splits[3], (FF, D), FF ** -0.5, 0.0625, ((0, 8), (1, 32)))
    return {"normed_input": normed_input, "cotangent": cotangent, "up_weight": up_weight, "down_weight": down_weight}


def reference(normed_input, cotangent, up_weight, down_weight):
    tokens = normed_input.shape[0]
    width = FF // FF_BLOCKS
    scale = lax.rsqrt(jnp.asarray(tokens, jnp.float32))

    def block(total, index):
        start = (index * width).astype(jnp.int32)
        up_block = lax.dynamic_slice_in_dim(up_weight, start, width, 1)
        down_block = lax.dynamic_slice_in_dim(down_weight, start, width, 0)
        pre = jnp.dot(normed_input, up_block, preferred_element_type=jnp.float32)
        rectified = jax.nn.relu(pre)
        act = (rectified * rectified).astype(jnp.bfloat16)
        act_grad = jnp.dot(cotangent, down_block.T, preferred_element_type=jnp.float32)
        pre_grad = (2.0 * rectified * act_grad).astype(jnp.bfloat16)
        down_part = jnp.dot(act.T, cotangent, preferred_element_type=jnp.float32) * scale
        up_part = jnp.dot(normed_input.T, pre_grad, preferred_element_type=jnp.float32) * scale
        partial_value = jnp.dot(pre_grad, up_block.T, preferred_element_type=jnp.float32).astype(jnp.bfloat16)
        partial_value = lax.optimization_barrier(partial_value)
        return (total + partial_value.astype(jnp.float32), (up_part, down_part))
    start_total = jnp.zeros(normed_input.shape, jnp.float32)
    total, parts = lax.scan(block, start_total, jnp.arange(FF_BLOCKS, dtype=jnp.int32))
    up_parts, down_parts = parts
    up_grad = jnp.moveaxis(up_parts, 0, 1).reshape(D, FF)
    down_grad = down_parts.reshape(FF, D)
    return (total.astype(jnp.bfloat16), up_grad, down_grad)
```

```python
import jax
import jax.numpy as jnp
from jax import lax
from jax.experimental import pallas as pl
from jax.experimental.pallas import tpu as pltpu
from jax.sharding import PartitionSpec as P

NX, NY, NZ = 4, 4, 8
D = 2048
TB = 256
FX = 512
HB = 256
DZ = 256
RY = 64
HALF = TB // 2
QUART = TB // 4
COPIES = 152
MESH = pl.DeviceIdType.MESH
BF16, F32 = jnp.bfloat16, jnp.float32


def nn(a, b):
    return lax.dot_general(a, b, (((1,), (0,)), ((), ())), preferred_element_type=F32)


def nt(a, b):
    return lax.dot_general(a, b, (((1,), (1,)), ((), ())), preferred_element_type=F32)


def kernel(
    x_in, c_in, up_in, dn_in, ig_out, ug_out, dg_out,
    xb, cb, w, xs, cs, uv, pg, tr, gt, gs, pb, rz, sz, fs_s, fs_r, g,
    ra, rb, sb, q1, rc, rd, sd, re, rf, sf, q2, rg, rh, sh, fp, rp,
    lsem, ssem, rsem,
):
    fs, tp = lax.axis_index("fs"), lax.axis_index("tp")
    z, y = lax.div(fs, NY), lax.rem(fs, NY)
    x, c = lax.div(tp, 2), lax.rem(tp, 2)
    o = 1 - c
    step = lambda a, k, n: lax.rem(a + (k % n), n)
    xr, xl, x2 = step(x, 1, NX), step(x, -1, NX), step(x, 2, NX)
    yr, yl, y2 = step(y, 1, NY), step(y, -1, NY), step(y, 2, NY)
    at = lambda ax, ay, az, ac: (az * NY + ay, ax * 2 + ac)
    XR, XL = at(xr, y, z, c), at(xl, y, z, c)
    YR, YL, Y2 = at(x, yr, z, c), at(x, yl, z, c), at(x, y2, z, c)
    ZR, ZL = at(x, y, step(z, 1, NZ), c), at(x, y, step(z, -1, NZ), c)
    PC = at(x, y, z, o)

    ids = iter(range(COPIES))
    sent = []

    def send(src, dst, where):
        i = next(ids)
        copy = pltpu.make_async_remote_copy(
            src_ref=src, dst_ref=dst, send_sem=ssem.at[i], recv_sem=rsem.at[i],
            device_id=where, device_id_type=MESH,
        )
        copy.start()
        sent.append(copy)
        return copy

    def cols(k, n):
        return pl.ds(pl.multiple_of(k * n, n), n)

    mine = lambda k: pl.ds(pl.multiple_of(x * FX + k * 256, 256), 256)
    loads = []
    for i, (src, dst) in enumerate((
        (x_in.at[cols(o, TB), :], xs),
        (c_in.at[cols(o, TB), :], cs),
        (x_in.at[cols(c, TB), :], xb.at[y, :, mine(c)]),
        (c_in.at[cols(c, TB), :], cb.at[y, :, mine(c)]),
        (up_in, uv.at[0]),
        (dn_in, uv.at[1]),
        (up_in.at[:, cols(y, HB)], w.at[0, c, pl.ds(pl.multiple_of(z * DZ + y * RY, RY), RY), :]),
        (dn_in.at[:, cols(y, HB)], w.at[1, c, pl.ds(pl.multiple_of(z * DZ + y * RY, RY), RY), :]),
    )):
        copy = pltpu.make_async_copy(src, dst, lsem.at[i])
        copy.start()
        loads.append(copy)

    barrier = pltpu.get_barrier_semaphore()
    peers = (XR, XL, YR, YL, Y2, ZR, ZL, PC)
    for peer in peers:
        pl.semaphore_signal(barrier, inc=1, device_id=peer, device_id_type=MESH)
    pl.semaphore_wait(barrier, len(peers))

    loads[1].wait()
    cop = send(cs, cb.at[y, :, mine(c)], PC)
    loads[0].wait()
    xop = send(xs, xb.at[y, :, mine(c)], PC)
    loads[4].wait()
    loads[5].wait()
    wrow = pl.ds(pl.multiple_of(z * DZ + y * RY, RY), RY)
    wops = []
    for ay, where in ((y2, Y2), (yr, YR), (yl, YL)):
        for u in range(2):
            wops.append(send(uv.at[u, :, cols(ay, HB)], w.at[u, c, wrow, :], where))

    def blk(buf, ay, ax, half=None):
        rows = slice(None) if half is None else pl.ds(half * HALF, HALF)
        return buf.at[ay, rows, cols(ax, FX)]

    def both(buf, ay, ax, ways, half=None):
        ref = blk(buf, ay, ax, half)
        return [send(ref, ref, way) for way in ways]

    XX, YY = (XR, XL), (YR, YL)
    loads[2].wait()
    loads[3].wait()
    cop.wait_recv()
    c_y = {"me": both(cb, y, x, YY)}
    xop.wait_recv()
    x_x = both(xb, y, x, XX)
    x_y = {"me": both(xb, y, x, YY)}
    c_x = {"me": both(cb, y, x, XX)}

    loads[6].wait()
    loads[7].wait()
    for op in wops:
        op.wait_recv()

    def zblk(u, az):
        return w.at[u, c, cols(az, DZ), :]

    wz = [[], []]
    wpc = []
    order = ([(0, 0), (1, 0), (0, 1), (1, 1), (0, 2), (1, 2), (0, 3)],
             [(1, 0), (0, 0), (1, 1), (0, 1), (1, 2), (0, 2), (1, 3)])

    def wsend(way, i):
        u, k = order[way][i]
        ref = zblk(u, step(z, -k if way == 0 else k, NZ))
        wz[way].append(send(ref, ref, (ZR, ZL)[way]))

    for i in range(2):
        for way in range(2):
            wsend(way, i)
    for u in range(2):
        wpc.append(send(zblk(u, z), zblk(u, z), PC))

    def warrive(i):
        for way in range(2):
            wz[way][i].wait_recv()
            u, k = order[way][i]
            if i + 2 < 7:
                wsend(way, i + 2)
            ref = zblk(u, step(z, -(k + 1) if way == 0 else k + 1, NZ))
            wpc.append(send(ref, ref, PC))

    def got(ops):
        for op in ops:
            op.wait_recv()

    def pass_x(ay, ops):
        ops[0].wait_recv()
        a = blk(cb, ay, xl, 0)
        first = send(a, a, XR)
        ops[1].wait_recv()
        b = blk(cb, ay, xr, 1)
        return [first, send(b, b, XL)]

    def pass_y(ax, ops):
        ops[0].wait_recv()
        a = blk(xb, yl, ax, 0)
        first = send(a, a, YR)
        ops[1].wait_recv()
        b = blk(xb, yr, ax, 1)
        return [first, send(b, b, YL)]

    x_x[0].wait_recv()
    a = blk(xb, y, xl, 0)
    fx = [send(a, a, XR)]
    x_x[1].wait_recv()
    b = blk(xb, y, xr, 1)
    fx.append(send(b, b, XL))
    c_y["me"][0].wait_recv()
    a = blk(cb, yl, x, 0)
    fc = [send(a, a, YR)]
    c_y["me"][1].wait_recv()
    b = blk(cb, yr, x, 1)
    fc.append(send(b, b, YL))
    warrive(0)
    warrive(1)
    fcx = {"me": pass_x(y, c_x["me"])}
    x_y["l"] = both(xb, y, xl, YY)
    c_x["l"] = both(cb, yl, x, XX)
    x_y["r"] = both(xb, y, xr, YY)
    c_x["r"] = both(cb, yr, x, XX)
    warrive(2)
    got(fx)
    x_y["2"] = both(xb, y, x2, YY)
    got(fc)
    warrive(3)
    warrive(4)
    fxy = {"me": pass_y(x, x_y["me"])}
    warrive(5)
    fcx["l"] = pass_x(yl, c_x["l"])
    fxy["l"] = pass_y(xl, x_y["l"])
    warrive(6)
    got(fcx["me"])
    got(wpc)

    def forward(ay):
        for h in range(2):
            pre = nn(xb[ay], w[0, h])
            act_grad = nn(cb[ay], w[1, h])
            rect = jnp.maximum(pre, 0.0)
            grad = 2.0 * rect * act_grad
            pg[:, h * HB:(h + 1) * HB] = grad.astype(BF16)
            tr[0, h * HB:(h + 1) * HB, :] = grad.T.astype(BF16)
            tr[1, h * HB:(h + 1) * HB, :] = (rect * rect).T.astype(BF16)

    def partial(ay):
        @pl.loop(0, NZ)
        def _(k):
            rows = cols(k, DZ)
            total = nt(pg[:, :HB], w[0, 0, rows, :]) + nt(pg[:, HB:], w[0, 1, rows, :])
            g[ay, :, rows] = total.astype(BF16)

    def weights(ay, first):
        for u, buf in ((0, xb), (1, cb)):
            @pl.loop(0, NZ)
            def _(k):
                term = nn(tr[u], buf[ay, :, cols(k, DZ)])
                gt[u, k] = term if first else gt[u, k] + term

    forward(y)
    weights(y, True)
    fcx["r"] = pass_x(yr, c_x["r"])
    fxy["r"] = pass_y(xr, x_y["r"])
    lo, hi = blk(cb, y2, x, 0), blk(cb, y2, x, 1)
    c_x["2"] = [send(lo, lo, XR), send(hi, hi, XL)]
    c_x["3"] = [send(hi, hi, XR), send(lo, lo, XL)]
    partial(y)
    fxy["2"] = pass_y(x2, x_y["2"])
    got(fcx["l"])
    forward(yl)
    fcx["2"] = pass_x(y2, c_x["2"])
    weights(yl, False)
    partial(yl)
    got(fcx["r"])
    forward(yr)
    weights(yr, False)
    partial(yr)
    got(c_x["3"])
    got(fcx["2"])
    for name in ("me", "l", "r", "2"):
        got(fxy[name])
    forward(y2)
    partial(y2)

    xw = lambda k: cols(k, FX)
    h1 = [send(g.at[y2, 0:64, :], ra.at[0], YR), send(g.at[y2, 64:128, :], ra.at[1], YL)]
    h2 = [send(g.at[:, 128:192, xw(x2)], re.at[0], XR), send(g.at[:, 192:256, xw(x2)], re.at[1], XL)]
    h1b = [send(g.at[yr, 64:128, :], rb.at[0, 64:128, :], YR),
           send(g.at[yl, 0:64, :], rb.at[1, 0:64, :], YL)]
    h2b = [send(g.at[:, 192:256, xw(xr)], rf.at[0, :, 64:128, :], XR),
           send(g.at[:, 128:192, xw(xl)], rf.at[1, :, 0:64, :], XL)]

    down = ([(0, 4), (1, 3), (0, 3), (1, 2), (0, 2), (1, 1), (0, 1)],
            [(1, 4), (0, 3), (1, 3), (0, 2), (1, 2), (0, 1), (1, 1)])
    todo = []
    for i in range(7):
        for way in range(2):
            u, k = down[way][i]
            todo.append((u, k if way == 0 else -k))
    todo += [(0, 0), (1, 0)]
    own, other = cols(c, HB), cols(o, HB)
    wsum = {}
    for u, k in todo:
        az = step(z, k, NZ)
        rhs = (xb, cb)[u][y2, :, cols(az, DZ)]
        gs[u, az] = (gt[u, az, other, :] + nn(tr[u, other, :], rhs)).astype(BF16)
        wsum[u, k % NZ] = send(gs.at[u, az], pb.at[u, az], PC)
        gt[u, az, own, :] = gt[u, az, own, :] + nn(tr[u, own, :], rhs)

    gz = [[], []]

    def total(u, k):
        az = step(z, k, NZ)
        wsum[u, k % NZ].wait_recv()
        return gt[u, az, own, :] + pb[u, az].astype(F32)

    def gsend(way, i):
        u, k = down[way][i]
        value = total(u, k if way == 0 else -k)
        if i >= 2:
            gz[way][i - 2].wait_recv()
            value = value + rz[way, i - 2].astype(F32)
        sz[way, i] = value.astype(BF16)
        gz[way].append(send(sz.at[way, i], rz.at[way, i], (ZR, ZL)[way]))

    for i in range(3):
        for way in range(2):
            gsend(way, i)
    h1[0].wait_recv()
    sb[0] = (g[yr, 0:64, :].astype(F32) + ra[0].astype(F32)).astype(BF16)
    h1c = [send(sb.at[0], rb.at[0, 0:64, :], YR)]
    h1[1].wait_recv()
    sb[1] = (g[yl, 64:128, :].astype(F32) + ra[1].astype(F32)).astype(BF16)
    h1c.append(send(sb.at[1], rb.at[1, 64:128, :], YL))
    h2[0].wait_recv()
    sf[0] = (g[:, 128:192, xw(xr)].astype(F32) + re[0].astype(F32)).astype(BF16)
    h2c = [send(sf.at[0], rf.at[0, :, 0:64, :], XR)]
    h2[1].wait_recv()
    sf[1] = (g[:, 192:256, xw(xl)].astype(F32) + re[1].astype(F32)).astype(BF16)
    h2c.append(send(sf.at[1], rf.at[1, :, 64:128, :], XL))
    for i in range(3, 7):
        for way in range(2):
            gsend(way, i)

    got(h1b)
    got(h1c)
    for k in range(NX):
        s = slice(k * FX, (k + 1) * FX)
        q1[k] = g[y, 0:128, s].astype(F32) + rb[0, :, s].astype(F32) + rb[1, :, s].astype(F32)
    sd[0] = q1[x2].astype(BF16)
    sd[1, 64:128] = q1[xr, 64:128, :].astype(BF16)
    sd[2, 0:64] = q1[xl, 0:64, :].astype(BF16)
    v1 = [send(sd.at[0, 0:64, :], rc.at[0], XR), send(sd.at[0, 64:128, :], rc.at[1], XL)]
    v1b = [send(sd.at[1, 64:128, :], rd.at[0, 64:128, :], XR),
           send(sd.at[2, 0:64, :], rd.at[1, 0:64, :], XL)]
    got(h2b)
    got(h2c)
    q2[...] = g[:, 128:256, xw(x)].astype(F32) + rf[0].astype(F32) + rf[1].astype(F32)
    sh[0] = q2[y2].astype(BF16)
    sh[1, 64:128] = q2[yr, 64:128, :].astype(BF16)
    sh[2, 0:64] = q2[yl, 0:64, :].astype(BF16)
    v2 = [send(sh.at[0, 0:64, :], rg.at[0], YR), send(sh.at[0, 64:128, :], rg.at[1], YL)]
    v2b = [send(sh.at[1, 64:128, :], rh.at[0, 64:128, :], YR),
           send(sh.at[2, 0:64, :], rh.at[1, 0:64, :], YL)]

    v1[0].wait_recv()
    sd[1, 0:64] = (q1[xr, 0:64, :] + rc[0].astype(F32)).astype(BF16)
    v1c = [send(sd.at[1, 0:64, :], rd.at[0, 0:64, :], XR)]
    v1[1].wait_recv()
    sd[2, 64:128] = (q1[xl, 64:128, :] + rc[1].astype(F32)).astype(BF16)
    v1c.append(send(sd.at[2, 64:128, :], rd.at[1, 64:128, :], XL))
    v2[0].wait_recv()
    sh[1, 0:64] = (q2[yr, 0:64, :] + rg[0].astype(F32)).astype(BF16)
    v2c = [send(sh.at[1, 0:64, :], rh.at[0, 0:64, :], YR)]
    v2[1].wait_recv()
    sh[2, 64:128] = (q2[yl, 64:128, :] + rg[1].astype(F32)).astype(BF16)
    v2c.append(send(sh.at[2, 64:128, :], rh.at[1, 64:128, :], YL))

    scale = 1.0 / 128.0
    ops = []
    for u, out in ((0, ug_out), (1, dg_out)):
        way = 1 - u
        gz[0][6 - u].wait_recv()
        gz[1][5 + u].wait_recv()
        value = total(u, 0) + rz[0, 6 - u].astype(F32) + rz[1, 5 + u].astype(F32)
        gt[u, z, own, :] = (value * scale).T
        for i, (ay, where) in enumerate(((y2, Y2), (yr, YR), (yl, YL))):
            rows = pl.ds(pl.multiple_of(c * HB + ay * RY, RY), RY)
            fs_s[u, i] = gt[u, z, rows, :].astype(BF16)
            ops.append(send(fs_s.at[u, i], fs_r.at[u, i], where))
        rows = pl.ds(pl.multiple_of(c * HB + y * RY, RY), RY)
        out[:, cols(y, HB)] = gt[u, z, rows, :]

    got(v1b)
    got(v1c)
    first = q1[x] + rd[0].astype(F32) + rd[1].astype(F32)
    q1[0] = first
    got(v2b)
    got(v2c)
    second = q2[y] + rh[0].astype(F32) + rh[1].astype(F32)
    q1[1] = second
    lane = cols(o, 256)
    fp[0:128] = q1[0, :, lane].astype(BF16)
    fp[128:256] = q1[1, :, lane].astype(BF16)
    last = send(fp, rp, PC)
    lane = cols(c, 256)
    row = pl.multiple_of(c * TB, TB)
    ig_out[pl.ds(row, 128), :] = q1[0, :, lane].astype(BF16)
    ig_out[pl.ds(row + 128, 128), :] = q1[1, :, lane].astype(BF16)
    n = 0
    for u, out in ((0, ug_out), (1, dg_out)):
        for i, ay in enumerate((y2, yl, yr)):
            ops[n].wait_recv()
            n += 1
            out[:, cols(ay, HB)] = fs_r[u, i].astype(F32)
    last.wait_recv()
    ig_out[cols(o, TB), :] = rp[...]
    for copy in sent:
        copy.wait_send()


def per_device(normed_input, cotangent, up_weight, down_weight):
    bf = lambda *s: pltpu.VMEM(s, BF16)
    f4 = lambda *s: pltpu.VMEM(s, F32)
    any_spec = pl.BlockSpec(memory_space=pl.ANY)
    vmem = pl.BlockSpec(memory_space=pltpu.VMEM)
    ig, ug, dg = pl.pallas_call(
        kernel,
        out_shape=(
            jax.ShapeDtypeStruct((2 * TB, 256), BF16),
            jax.ShapeDtypeStruct((RY, 4 * HB), F32),
            jax.ShapeDtypeStruct((RY, 4 * HB), F32),
        ),
        in_specs=[any_spec] * 4,
        out_specs=(vmem,) * 3,
        scratch_shapes=[
            bf(NY, TB, D), bf(NY, TB, D),
            bf(2, 2, D, HB),
            bf(TB, 256), bf(TB, 256),
            bf(2, RY, 4 * HB),
            bf(TB, 2 * HB),
            bf(2, 2 * HB, TB),
            f4(2, NZ, 2 * HB, DZ),
            bf(2, NZ, HB, DZ), bf(2, NZ, HB, DZ),
            bf(2, 7, HB, DZ), bf(2, 7, HB, DZ),
            bf(2, 3, RY, HB), bf(2, 3, RY, HB),
            bf(NY, TB, D),
            bf(2, 64, D), bf(2, 128, D), bf(2, 64, D),
            f4(NX, 128, FX),
            bf(2, 64, FX), bf(2, 128, FX), bf(3, 128, FX),
            bf(2, NY, 64, FX), bf(2, NY, 128, FX), bf(2, NY, 64, FX),
            f4(NY, 128, FX),
            bf(2, 64, FX), bf(2, 128, FX), bf(3, 128, FX),
            bf(TB, 256), bf(TB, 256),
            pltpu.SemaphoreType.DMA((8,)),
            pltpu.SemaphoreType.DMA((COPIES,)),
            pltpu.SemaphoreType.DMA((COPIES,)),
        ],
        compiler_params=pltpu.CompilerParams(
            collective_id=0, has_side_effects=True, vmem_limit_bytes=60 * 1024 * 1024
        ),
    )(normed_input, cotangent, up_weight, down_weight.T)
    return ig, ug, dg.T


def solution(mesh):
    return jax.shard_map(
        per_device, mesh=mesh,
        in_specs=(P("fs", "tp"), P("fs", "tp"), P("fs", "tp"), P("tp", "fs")),
        out_specs=(P("fs", "tp"), P("fs", "tp"), P("tp", "fs")),
        check_vma=False,
    )
```

```python
import jax
import jax.numpy as jnp
from jax import lax
from jax.experimental import pallas as pl
from jax.experimental.pallas import tpu as pltpu
from jax.sharding import PartitionSpec as P

NX, NY, NZ = 4, 4, 8
D = 2048
TB = 256
FX = 512
HB = 256
DZ = 256
RY = 64
HALF = TB // 2
QUART = TB // 4
COPIES = 160
MESH = pl.DeviceIdType.MESH
BF16, F32 = jnp.bfloat16, jnp.float32


def nn(a, b):
    return lax.dot_general(a, b, (((1,), (0,)), ((), ())), preferred_element_type=F32)


def nt(a, b):
    return lax.dot_general(a, b, (((1,), (1,)), ((), ())), preferred_element_type=F32)


def kernel(
    x_in, c_in, up_in, dn_in, ow, og,
    xb, cb, w, xs, cs, uv, pg, tr, acc, gt, gs, pb, rz, sz, fs_s, g,
    ra, rb, sb, q1, rc, rd, sd, re, rf, sf, q2, rg, rh, sh, fp,
    lsem, ssem, rsem,
):
    fs, tp = lax.axis_index("fs"), lax.axis_index("tp")
    z, y = lax.div(fs, NY), lax.rem(fs, NY)
    x, c = lax.div(tp, 2), lax.rem(tp, 2)
    o = 1 - c
    step = lambda a, k, n: lax.rem(a + (k % n), n)
    xr, xl, x2 = step(x, 1, NX), step(x, -1, NX), step(x, 2, NX)
    yr, yl, y2 = step(y, 1, NY), step(y, -1, NY), step(y, 2, NY)
    at = lambda ax, ay, az, ac: (az * NY + ay, ax * 2 + ac)
    XR, XL = at(xr, y, z, c), at(xl, y, z, c)
    YR, YL, Y2 = at(x, yr, z, c), at(x, yl, z, c), at(x, y2, z, c)
    ZR, ZL = at(x, y, step(z, 1, NZ), c), at(x, y, step(z, -1, NZ), c)
    PC = at(x, y, z, o)
    ME, L, R, OPP = range(4)

    ids = iter(range(COPIES))
    sent = []

    def send(src, dst, where):
        i = next(ids)
        copy = pltpu.make_async_remote_copy(
            src_ref=src, dst_ref=dst, send_sem=ssem.at[i], recv_sem=rsem.at[i],
            device_id=where, device_id_type=MESH,
        )
        copy.start()
        sent.append(copy)
        return copy

    def got(ops):
        for op in ops:
            op.wait_recv()

    def cols(k, n):
        return pl.ds(pl.multiple_of(k * n, n), n)

    mine = pl.ds(pl.multiple_of(x * FX + c * 256, 256), 256)
    wrow = pl.ds(pl.multiple_of(z * DZ + y * RY, RY), RY)
    loads = []
    for i, (src, dst) in enumerate((
        (c_in.at[cols(o, TB), :], cs),
        (x_in.at[cols(o, TB), :], xs),
        (up_in, uv.at[0]),
        (dn_in, uv.at[1]),
        (c_in.at[cols(c, TB), :], cb.at[0:TB, mine]),
        (x_in.at[cols(c, TB), :], xb.at[0:TB, mine]),
        (up_in.at[:, cols(y, HB)], w.at[0, wrow, 0:HB]),
        (dn_in.at[:, cols(y, HB)], w.at[1, wrow, 0:HB]),
    )):
        copy = pltpu.make_async_copy(src, dst, lsem.at[i])
        copy.start()
        loads.append(copy)

    barrier = pltpu.get_barrier_semaphore()
    peers = (XR, XL, YR, YL, Y2, ZR, ZL, PC)
    for peer in peers:
        pl.semaphore_signal(barrier, inc=1, device_id=peer, device_id_type=MESH)
    pl.semaphore_wait(barrier, len(peers))

    loads[0].wait()
    cop = send(cs, cb.at[0:TB, mine], PC)
    loads[1].wait()
    xop = send(xs, xb.at[0:TB, mine], PC)
    loads[2].wait()
    loads[3].wait()
    wops = []
    for ay, where in ((y2, Y2), (yr, YR), (yl, YL)):
        for u in range(2):
            wops.append(send(uv.at[u, :, cols(ay, HB)], w.at[u, wrow, 0:HB], where))

    def blk(buf, slot, ax, half=None):
        if half is None:
            return buf.at[slot * TB:(slot + 1) * TB, cols(ax, FX)]
        return buf.at[slot * TB + half * HALF:slot * TB + (half + 1) * HALF, cols(ax, FX)]

    def over_x(buf, slot, ax):
        ref = blk(buf, slot, ax)
        return [send(ref, ref, XR), send(ref, ref, XL)]

    def over_y(buf, ax):
        ref = blk(buf, ME, ax)
        return [send(ref, blk(buf, L, ax), YR), send(ref, blk(buf, R, ax), YL)]

    def pass_x(buf, slot, ops):
        ops[0].wait_recv()
        a = blk(buf, slot, xl, 0)
        first = send(a, a, XR)
        ops[1].wait_recv()
        b = blk(buf, slot, xr, 1)
        return [first, send(b, b, XL)]

    def pass_y(buf, ax, ops):
        ops[0].wait_recv()
        first = send(blk(buf, L, ax, 0), blk(buf, OPP, ax, 0), YR)
        ops[1].wait_recv()
        return [first, send(blk(buf, R, ax, 1), blk(buf, OPP, ax, 1), YL)]

    loads[4].wait()
    loads[5].wait()
    cop.wait_recv()
    c_y = over_y(cb, x)
    xop.wait_recv()
    x_x = over_x(xb, ME, x)
    x_y = {"me": over_y(xb, x)}
    c_x = {"me": over_x(cb, ME, x)}

    loads[6].wait()
    loads[7].wait()
    got(wops)

    wz = [[], []]
    wpc = []
    order = ([(0, 0), (1, 0), (0, 1), (1, 1), (0, 2), (1, 2), (0, 3)],
             [(1, 0), (0, 0), (1, 1), (0, 1), (1, 2), (0, 2), (1, 3)])

    def wsend(way, i):
        u, k = order[way][i]
        ref = w.at[u, cols(step(z, -k if way == 0 else k, NZ), DZ), 0:HB]
        wz[way].append(send(ref, ref, (ZR, ZL)[way]))

    def wpair(u, k):
        rows = cols(step(z, k, NZ), DZ)
        wpc.append(send(w.at[u, rows, 0:HB], w.at[u, rows, HB:2 * HB], PC))

    for i in range(2):
        for way in range(2):
            wsend(way, i)
    for u in range(2):
        wpair(u, 0)

    def warrive(i):
        for way in range(2):
            wz[way][i].wait_recv()
            u, k = order[way][i]
            if i + 2 < 7:
                wsend(way, i + 2)
            wpair(u, -(k + 1) if way == 0 else k + 1)

    fx = pass_x(xb, ME, x_x)
    warrive(0)
    fc = pass_y(cb, x, c_y)
    x_y["l"] = over_y(xb, xl)
    x_y["r"] = over_y(xb, xr)
    warrive(1)
    fcx = {"me": pass_x(cb, ME, c_x["me"])}
    c_x["l"] = over_x(cb, L, x)
    c_x["r"] = over_x(cb, R, x)
    warrive(2)
    got(fx)
    x_y["2"] = over_y(xb, x2)
    warrive(3)
    fxy = {"me": pass_y(xb, x, x_y["me"])}
    got(fc)
    warrive(4)
    warrive(5)
    fcx["l"] = pass_x(cb, L, c_x["l"])
    fxy["l"] = pass_y(xb, xl, x_y["l"])
    warrive(6)
    got(fcx["me"])
    got(wpc)

    def forward(slot, pre=None, act_grad=None):
        rows = slice(slot * TB, (slot + 1) * TB)
        for h in range(2):
            s = slice(h * HB, (h + 1) * HB)
            pre = nn(xb[rows], w[0, :, s])
            act_grad = nn(cb[rows], w[1, :, s])
            finish(slot, s, pre, act_grad)

    def finish(slot, s, pre, act_grad):
        rows = slice(slot * TB, (slot + 1) * TB)
        rect = jnp.maximum(pre, 0.0)
        grad = 2.0 * rect * act_grad
        pg[rows, s] = grad.astype(BF16)
        tr[0, s, rows] = grad.T.astype(BF16)
        tr[1, s, rows] = (rect * rect).T.astype(BF16)

    def partial(lo, hi):
        rows = slice(lo * TB, hi * TB)

        @pl.loop(0, NZ, unroll=2)
        def _(k):
            lane = cols(k, DZ)
            g[rows, lane] = nt(pg[rows, :], w[0, lane, :]).astype(BF16)

    forward(ME)
    fcx["r"] = pass_x(cb, R, c_x["r"])
    c2 = [send(blk(cb, OPP, x, h), blk(cb, OPP, x, h), (XR, XL)[h]) for h in range(2)]
    c3 = [send(blk(cb, OPP, x, 1 - h), blk(cb, OPP, x, 1 - h), (XR, XL)[h]) for h in range(2)]
    partial(ME, L)
    fxy["r"] = pass_y(xb, xr, x_y["r"])
    fxy["2"] = pass_y(xb, x2, x_y["2"])
    got(fcx["l"])
    forward(L)
    fcx["2"] = pass_x(cb, OPP, c2)
    got(fcx["r"])
    forward(R)
    partial(L, OPP)

    def part(slot, r, n, lane=slice(None)):
        return g.at[slot * TB + r:slot * TB + r + n, lane]

    h1b = [send(part(R, 64, 64), rb.at[0, 64:128, :], YR),
           send(part(L, 0, 64), rb.at[1, 0:64, :], YL)]
    h2, h2b = {}, {}
    far, right, left = cols(x2, FX), cols(xr, FX), cols(xl, FX)

    def first_x(slot):
        h2[slot] = [send(part(slot, 128, 64, far), re.at[0, slot], XR),
                    send(part(slot, 192, 64, far), re.at[1, slot], XL)]

    def next_x(slot):
        h2b[slot] = [send(part(slot, 192, 64, right), rf.at[0, slot, 64:128], XR),
                     send(part(slot, 128, 64, left), rf.at[1, slot, 0:64], XL)]

    def last_x(slot):
        h2[slot][0].wait_recv()
        sf[0, slot] = (part(slot, 128, 64, right)[...].astype(F32) + re[0, slot].astype(F32)).astype(BF16)
        h2b[slot].append(send(sf.at[0, slot], rf.at[0, slot, 0:64], XR))
        h2[slot][1].wait_recv()
        sf[1, slot] = (part(slot, 192, 64, left)[...].astype(F32) + re[1, slot].astype(F32)).astype(BF16)
        h2b[slot].append(send(sf.at[1, slot], rf.at[1, slot, 64:128], XL))

    for slot in (ME, L, R):
        first_x(slot)
    for slot in (ME, L, R):
        next_x(slot)

    for u, buf in ((0, xb), (1, cb)):
        @pl.loop(0, NZ, unroll=2)
        def _(k):
            gt[u, k] = nn(tr[u, :, 0:3 * TB], buf[0:3 * TB, cols(k, DZ)])

    orow = slice(OPP * TB, OPP * TB + TB)
    got(c3)
    got(fcx["2"])
    for h in range(2):
        s = slice(h * HB, (h + 1) * HB)
        acc[1, :, s] = nn(cb[orow], w[1, :, s])
    got(fxy["me"] + fxy["l"] + fxy["r"])
    for n, ax in enumerate((x, xl, xr)):
        lane = cols(ax, FX)
        term = nn(xb[orow, lane], w[0, lane, :])
        acc[0] = term if n == 0 else acc[0] + term
    got(fxy["2"])
    pre = acc[0] + nn(xb[orow, far], w[0, far, :])
    finish(OPP, slice(0, 2 * HB), pre, acc[1])

    down = ([(0, 4), (1, 3), (0, 3), (1, 2), (0, 2), (1, 1), (0, 1)],
            [(1, 4), (0, 3), (1, 3), (0, 2), (1, 2), (0, 1), (1, 1)])
    todo = []
    for i in range(7):
        for way in range(2):
            u, k = down[way][i]
            todo.append((u, k if way == 0 else -k))
    todo += [(0, 0), (1, 0)]
    wsum = {}

    def chunk(u, k):
        az = step(z, k, NZ)
        value = gt[u, az] + nn(tr[u, :, 3 * TB:], (xb, cb)[u][orow, cols(az, DZ)])
        gs[u, az] = value[HB:].astype(BF16)
        wsum[u, k % NZ] = send(gs.at[u, az], pb.at[u, az], PC)
        gt[u, az, 0:HB] = value[:HB]

    gz = [[], []]

    def total(u, k):
        az = step(z, k, NZ)
        wsum[u, k % NZ].wait_recv()
        return gt[u, az, 0:HB] + pb[u, az].astype(F32)

    def gsend(i):
        for way in range(2):
            u, k = down[way][i]
            value = total(u, k if way == 0 else -k)
            if i >= 2:
                gz[way][i - 2].wait_recv()
                value = value + rz[way, i - 2].astype(F32)
            sz[way, i] = value.astype(BF16)
            gz[way].append(send(sz.at[way, i], rz.at[way, i], (ZR, ZL)[way]))

    for u, k in todo[:4]:
        chunk(u, k)
    gsend(0)
    partial(OPP, OPP + 1)
    h1 = [send(part(OPP, 0, 64), ra.at[0], YR), send(part(OPP, 64, 64), ra.at[1], YL)]
    first_x(OPP)
    next_x(OPP)
    gsend(1)
    for slot in (ME, L, R):
        last_x(slot)
    for u, k in todo[4:]:
        chunk(u, k)
    gsend(2)
    h1[0].wait_recv()
    sb[0] = (part(R, 0, 64)[...].astype(F32) + ra[0].astype(F32)).astype(BF16)
    h1c = [send(sb.at[0], rb.at[0, 0:64, :], YR)]
    h1[1].wait_recv()
    sb[1] = (part(L, 64, 64)[...].astype(F32) + ra[1].astype(F32)).astype(BF16)
    h1c.append(send(sb.at[1], rb.at[1, 64:128, :], YL))
    last_x(OPP)
    gsend(3)
    gsend(4)

    for slot in range(4):
        got(h2b[slot])
    here = cols(x, FX)
    for slot in range(4):
        q2[slot] = (part(slot, 128, 128, here)[...].astype(F32)
                    + rf[0, slot].astype(F32) + rf[1, slot].astype(F32))
    sh[0] = q2[OPP].astype(BF16)
    sh[1, 64:128] = q2[R, 64:128, :].astype(BF16)
    sh[2, 0:64] = q2[L, 0:64, :].astype(BF16)
    v2 = [send(sh.at[0, 0:64, :], rg.at[0], YR), send(sh.at[0, 64:128, :], rg.at[1], YL)]
    v2b = [send(sh.at[1, 64:128, :], rh.at[0, 64:128, :], YR),
           send(sh.at[2, 0:64, :], rh.at[1, 0:64, :], YL)]
    got(h1b)
    got(h1c)
    for k in range(NX):
        s = slice(k * FX, (k + 1) * FX)
        q1[k] = g[0:128, s].astype(F32) + rb[0, :, s].astype(F32) + rb[1, :, s].astype(F32)
    sd[0] = q1[x2].astype(BF16)
    sd[1, 64:128] = q1[xr, 64:128, :].astype(BF16)
    sd[2, 0:64] = q1[xl, 0:64, :].astype(BF16)
    v1 = [send(sd.at[0, 0:64, :], rc.at[0], XR), send(sd.at[0, 64:128, :], rc.at[1], XL)]
    v1b = [send(sd.at[1, 64:128, :], rd.at[0, 64:128, :], XR),
           send(sd.at[2, 0:64, :], rd.at[1, 0:64, :], XL)]
    gsend(5)
    v2[0].wait_recv()
    sh[1, 0:64] = (q2[R, 0:64, :] + rg[0].astype(F32)).astype(BF16)
    v2c = [send(sh.at[1, 0:64, :], rh.at[0, 0:64, :], YR)]
    v2[1].wait_recv()
    sh[2, 64:128] = (q2[L, 64:128, :] + rg[1].astype(F32)).astype(BF16)
    v2c.append(send(sh.at[2, 64:128, :], rh.at[1, 64:128, :], YL))
    v1[0].wait_recv()
    sd[1, 0:64] = (q1[xr, 0:64, :] + rc[0].astype(F32)).astype(BF16)
    v1c = [send(sd.at[1, 0:64, :], rd.at[0, 0:64, :], XR)]
    v1[1].wait_recv()
    sd[2, 64:128] = (q1[xl, 64:128, :] + rc[1].astype(F32)).astype(BF16)
    v1c.append(send(sd.at[2, 64:128, :], rd.at[1, 64:128, :], XL))
    gsend(6)
    own, other = cols(c, 256), cols(o, 256)
    ends = []

    def finish_rows(r, value, n):
        q1[n] = value
        fp[0, r:r + 128] = q1[n, :, other].astype(BF16)
        fp[1, r:r + 128] = q1[n, :, own].astype(BF16)
        row = pl.ds(pl.multiple_of(c * TB + r, 128), 128)
        ends.append(send(fp.at[0, r:r + 128], og.at[row, :], PC))
        copy = pltpu.make_async_copy(fp.at[1, r:r + 128], og.at[row, :], lsem.at[8 + n])
        copy.start()
        return copy

    got(v1b)
    got(v1c)
    stores = [finish_rows(0, q1[x] + rd[0].astype(F32) + rd[1].astype(F32), 0)]
    got(v2b)
    got(v2c)
    stores.append(finish_rows(128, q2[ME] + rh[0].astype(F32) + rh[1].astype(F32), 1))

    scale = 1.0 / 128.0
    ops = []
    for u in range(2):
        value = total(u, 0)
        gz[0][6 - u].wait_recv()
        gz[1][5 + u].wait_recv()
        value = value + rz[0, 6 - u].astype(F32) + rz[1, 5 + u].astype(F32)
        fs_s[u] = (value * scale).T.astype(BF16)
        there = cols(y, HB)
        for ay, where in ((y2, Y2), (yr, YR), (yl, YL)):
            ops.append(send(fs_s.at[u, cols(ay, RY), :], ow.at[u, :, there], where))
        copy = pltpu.make_async_copy(fs_s.at[u, cols(y, RY), :], ow.at[u, :, there], lsem.at[10 + u])
        copy.start()
        stores.append(copy)
    got(ops)
    got(ends)
    for copy in stores:
        copy.wait()
    for copy in sent:
        copy.wait_send()


def finisher(ow, og, ig_out, ug_out, dg_out, wv, gv, fv, sem):
    loads = [pltpu.make_async_copy(ow.at[u], wv.at[u], sem.at[u]) for u in range(2)]
    loads.append(pltpu.make_async_copy(og, gv, sem.at[2]))
    for copy in loads:
        copy.start()
    stores = []
    for u, out in ((0, ug_out), (1, dg_out)):
        loads[u].wait()
        fv[u] = wv[u].astype(F32)
        stores.append(pltpu.make_async_copy(fv.at[u], out, sem.at[3 + u]))
        stores[-1].start()
    loads[2].wait()
    stores.append(pltpu.make_async_copy(gv, ig_out, sem.at[5]))
    stores[-1].start()
    for copy in stores:
        copy.wait()


def per_device(normed_input, cotangent, up_weight, down_weight):
    bf = lambda *s: pltpu.VMEM(s, BF16)
    f4 = lambda *s: pltpu.VMEM(s, F32)
    hbm = pl.BlockSpec(memory_space=pl.ANY)
    shape = jax.ShapeDtypeStruct
    ow, og = pl.pallas_call(
        kernel,
        out_shape=(shape((2, RY, 4 * HB), BF16), shape((2 * TB, 256), BF16)),
        in_specs=[hbm] * 4,
        out_specs=(hbm,) * 2,
        scratch_shapes=[
            bf(NY * TB, D), bf(NY * TB, D),
            bf(2, D, 2 * HB),
            bf(TB, 256), bf(TB, 256),
            bf(2, RY, 4 * HB),
            bf(NY * TB, 2 * HB),
            bf(2, 2 * HB, NY * TB),
            f4(2, TB, 2 * HB),
            f4(2, NZ, 2 * HB, DZ),
            bf(2, NZ, HB, DZ), bf(2, NZ, HB, DZ),
            bf(2, 7, HB, DZ), bf(2, 7, HB, DZ),
            bf(2, DZ, HB),
            bf(NY * TB, D),
            bf(2, 64, D), bf(2, 128, D), bf(2, 64, D),
            f4(NX, 128, FX),
            bf(2, 64, FX), bf(2, 128, FX), bf(3, 128, FX),
            bf(2, NY, 64, FX), bf(2, NY, 128, FX), bf(2, NY, 64, FX),
            f4(NY, 128, FX),
            bf(2, 64, FX), bf(2, 128, FX), bf(3, 128, FX),
            bf(2, TB, 256),
            pltpu.SemaphoreType.DMA((12,)),
            pltpu.SemaphoreType.DMA((COPIES,)),
            pltpu.SemaphoreType.DMA((COPIES,)),
        ],
        compiler_params=pltpu.CompilerParams(
            collective_id=0, has_side_effects=True, vmem_limit_bytes=60 * 1024 * 1024
        ),
    )(normed_input, cotangent, up_weight, down_weight.T)
    ig, ug, dg = pl.pallas_call(
        finisher,
        out_shape=(shape((2 * TB, 256), BF16), shape((RY, 4 * HB), F32), shape((RY, 4 * HB), F32)),
        in_specs=[hbm] * 2,
        out_specs=(hbm,) * 3,
        scratch_shapes=[
            bf(2, RY, 4 * HB), bf(2 * TB, 256), f4(2, RY, 4 * HB), pltpu.SemaphoreType.DMA((6,)),
        ],
    )(ow, og)
    return ig, ug, dg.T


def solution(mesh):
    return jax.shard_map(
        per_device, mesh=mesh,
        in_specs=(P("fs", "tp"), P("fs", "tp"), P("fs", "tp"), P("tp", "fs")),
        out_specs=(P("fs", "tp"), P("fs", "tp"), P("tp", "fs")),
        check_vma=False,
    )
```

```python
import math

import jax
import jax.numpy as jnp
from jax import lax
from jax.experimental import pallas as pl
from jax.experimental.pallas import tpu as pltpu
from jax.sharding import PartitionSpec as P

NX, NY, NZ = 4, 4, 8
D = 2048
TB = 256
FX = 512
HB = 256
DZ = 256
RY = 64
HALF = TB // 2
SPLIT = (128, 112)
SENDS, RECVS = 10, 72
MESH = pl.DeviceIdType.MESH
BF16, F32 = jnp.bfloat16, jnp.float32


def nn(a, b):
    return lax.dot_general(a, b, (((1,), (0,)), ((), ())), preferred_element_type=F32)


def nt(a, b):
    return lax.dot_general(a, b, (((1,), (1,)), ((), ())), preferred_element_type=F32)


def kernel(
    x_in, c_in, up_in, dn_in, ow, og,
    xb, cb, w, xs, cs, uv, pg, tr, acc, gt, gs, pb, rz, sz, fs_s, g,
    ra, rb, sb, q1, rc, rd, sd, re, rf, sf, q2, rg, rh, sh, fp,
    lsem, ssem, rsem,
):
    fs, tp = lax.axis_index("fs"), lax.axis_index("tp")
    z, y = lax.div(fs, NY), lax.rem(fs, NY)
    x, c = lax.div(tp, 2), lax.rem(tp, 2)
    o = 1 - c
    step = lambda a, k, n: lax.rem(a + (k % n), n)
    xr, xl, x2 = step(x, 1, NX), step(x, -1, NX), step(x, 2, NX)
    yr, yl, y2 = step(y, 1, NY), step(y, -1, NY), step(y, 2, NY)
    at = lambda ax, ay, az, ac: (az * NY + ay, ax * 2 + ac)
    XR, XL = at(xr, y, z, c), at(xl, y, z, c)
    YR, YL, Y2 = at(x, yr, z, c), at(x, yl, z, c), at(x, y2, z, c)
    ZR, ZL = at(x, y, step(z, 1, NZ), c), at(x, y, step(z, -1, NZ), c)
    PC = at(x, y, z, o)
    ME, L, R, OPP = range(4)

    arrivals = iter(range(RECVS))
    groups = []
    SPAN = 4 << 20

    def size(ref):
        return math.prod(ref.shape) * 2

    def span(count):
        return xb.at[0:count // (2 * D), :]

    class Batch:
        def __init__(self):
            self.sem, self.bytes = rsem.at[next(arrivals)], 0

        def send(self, src, dst, where, small=False):
            n = size(src)
            at = next((k for k, g in enumerate(groups) if g[1] == small and g[0] + n <= SPAN), None)
            if at is None:
                at = len(groups)
                groups.append([0, small])
            groups[at][0] += n
            self.bytes += n
            pltpu.make_async_remote_copy(
                src_ref=src, dst_ref=dst, send_sem=ssem.at[at], recv_sem=self.sem,
                device_id=where, device_id_type=MESH,
            ).start()
            return self

        def wait(self):
            ref = span(self.bytes)
            pltpu.make_async_copy(ref, ref, self.sem).wait()

    def send(src, dst, where):
        return Batch().send(src, dst, where)

    def cols(k, n):
        return pl.ds(pl.multiple_of(k * n, n), n)

    mine = pl.ds(pl.multiple_of(x * FX + c * 256, 256), 256)
    wrow = pl.ds(pl.multiple_of(z * DZ + y * RY, RY), RY)
    loads = []
    for i, pairs in enumerate((
        ((c_in.at[cols(o, TB), :], cs),),
        ((x_in.at[cols(o, TB), :], xs),),
        ((up_in, uv.at[0]), (dn_in, uv.at[1])),
        ((c_in.at[cols(c, TB), :], cb.at[0:TB, mine]), (x_in.at[cols(c, TB), :], xb.at[0:TB, mine])),
        ((up_in.at[:, cols(y, HB)], w.at[0, wrow, 0:HB]),
         (dn_in.at[:, cols(y, HB)], w.at[1, wrow, 0:HB])),
    )):
        for src, dst in pairs:
            pltpu.make_async_copy(src, dst, lsem.at[i]).start()
        ref = span(sum(size(dst) for _, dst in pairs))
        loads.append(pltpu.make_async_copy(ref, ref, lsem.at[i]))

    barrier = pltpu.get_barrier_semaphore()
    peers = (XR, XL, YR, YL, Y2, ZR, ZL, PC)
    for peer in peers:
        pl.semaphore_signal(barrier, inc=1, device_id=peer, device_id_type=MESH)
    pl.semaphore_wait(barrier, len(peers))

    loads[0].wait()
    cop = send(cs, cb.at[0:TB, mine], PC)
    loads[1].wait()
    xop = send(xs, xb.at[0:TB, mine], PC)
    loads[2].wait()
    wops = Batch()
    for ay, where in ((y2, Y2), (yr, YR), (yl, YL)):
        for u in range(2):
            wops.send(uv.at[u, :, cols(ay, HB)], w.at[u, wrow, 0:HB], where, small=True)

    def blk(buf, slot, ax, lo=0, hi=TB):
        return buf.at[slot * TB + lo:slot * TB + hi, cols(ax, FX)]

    def over_x(buf, slot, ax):
        ref = blk(buf, slot, ax)
        return send(ref, ref, XR).send(ref, ref, XL)

    def over_y(buf, ax):
        ref = blk(buf, ME, ax)
        return send(ref, blk(buf, L, ax), YR).send(ref, blk(buf, R, ax), YL)

    def pass_x(buf, slot, batch, out=None):
        batch.wait()
        cut = SPLIT[0]
        a, b = blk(buf, slot, xl, 0, cut), blk(buf, slot, xr, cut)
        return (out or Batch()).send(a, a, XR).send(b, b, XL)

    def pass_y(buf, ax, batch, out=None):
        batch.wait()
        cut = SPLIT[1]
        out = out or Batch()
        out.send(blk(buf, L, ax, 0, cut), blk(buf, OPP, ax, 0, cut), YR)
        return out.send(blk(buf, R, ax, cut), blk(buf, OPP, ax, cut), YL)

    loads[3].wait()
    cop.wait()
    c_y = over_y(cb, x)
    xop.wait()
    x_x = over_x(xb, ME, x)
    x_y = {"me": over_y(xb, x)}
    c_x = {"me": over_x(cb, ME, x)}

    loads[4].wait()
    wops.wait()

    wz = []
    wpc = Batch()
    order = ([(0, 0), (1, 0), (0, 1), (1, 1), (0, 2), (1, 2), (0, 3)],
             [(1, 0), (0, 0), (1, 1), (0, 1), (1, 2), (0, 2), (1, 3)])

    def wsend(i):
        batch = Batch()
        for way in range(2):
            u, k = order[way][i]
            ref = w.at[u, cols(step(z, -k if way == 0 else k, NZ), DZ), 0:HB]
            batch.send(ref, ref, (ZR, ZL)[way])
        wz.append(batch)

    def wpair(u, k):
        rows = cols(step(z, k, NZ), DZ)
        wpc.send(w.at[u, rows, 0:HB], w.at[u, rows, HB:2 * HB], PC)

    wsend(0)
    wsend(1)
    for u in range(2):
        wpair(u, 0)

    def warrive(i):
        wz[i].wait()
        if i + 2 < 7:
            wsend(i + 2)
        for way in range(2):
            u, k = order[way][i]
            wpair(u, -(k + 1) if way == 0 else k + 1)

    fx = pass_x(xb, ME, x_x)
    warrive(0)
    fc = pass_y(cb, x, c_y)
    x_y["l"] = over_y(xb, xl)
    x_y["r"] = over_y(xb, xr)
    warrive(1)
    fcx = {"me": pass_x(cb, ME, c_x["me"])}
    c_x["l"] = over_x(cb, L, x)
    c_x["r"] = over_x(cb, R, x)
    warrive(2)
    fx.wait()
    x_y["2"] = over_y(xb, x2)
    warrive(3)
    fxy = pass_y(xb, x, x_y["me"])
    fc.wait()
    warrive(4)
    warrive(5)
    fcx["l"] = pass_x(cb, L, c_x["l"])
    pass_y(xb, xl, x_y["l"], fxy)
    warrive(6)
    fcx["me"].wait()
    wpc.wait()

    def forward(slot):
        rows = slice(slot * TB, (slot + 1) * TB)
        for h in range(2):
            s = slice(h * HB, (h + 1) * HB)
            pre = nn(xb[rows], w[0, :, s])
            act_grad = nn(cb[rows], w[1, :, s])
            finish(slot, s, pre, act_grad)

    def finish(slot, s, pre, act_grad):
        rows = slice(slot * TB, (slot + 1) * TB)
        rect = jnp.maximum(pre, 0.0)
        grad = 2.0 * rect * act_grad
        pg[rows, s] = grad.astype(BF16)
        tr[0, s, rows] = grad.T.astype(BF16)
        tr[1, s, rows] = (rect * rect).T.astype(BF16)

    def partial(lo, hi):
        rows = slice(lo * TB, hi * TB)

        @pl.loop(0, NZ, unroll=2)
        def _(k):
            lane = cols(k, DZ)
            g[rows, lane] = nt(pg[rows, :], w[0, lane, :]).astype(BF16)

    forward(ME)
    fcx["r"] = pass_x(cb, R, c_x["r"])
    lo, hi = blk(cb, OPP, x, 0, HALF), blk(cb, OPP, x, HALF)
    c2 = send(lo, lo, XR).send(hi, hi, XL)
    c3 = send(hi, hi, XR).send(lo, lo, XL)
    partial(ME, L)
    pass_y(xb, xr, x_y["r"], fxy)
    fxy2 = pass_y(xb, x2, x_y["2"])
    fcx["l"].wait()
    forward(L)
    fcx["r"].wait()
    forward(R)
    fcx["2"] = pass_x(cb, OPP, c2)
    partial(L, OPP)

    def part(slot, r, n, lane=slice(None)):
        return g.at[slot * TB + r:slot * TB + r + n, lane]

    h1b = Batch()
    h1b.send(part(R, 64, 64), rb.at[0, 64:128, :], YR)
    h1b.send(part(L, 0, 64), rb.at[1, 0:64, :], YL)
    far, right, left = cols(x2, FX), cols(xr, FX), cols(xl, FX)
    h2, h2b = {}, Batch()

    def first_x(slots):
        batch = Batch()
        for slot in slots:
            batch.send(part(slot, 128, 64, far), re.at[0, slot], XR)
            batch.send(part(slot, 192, 64, far), re.at[1, slot], XL)
            h2[slot] = batch
        return batch

    def next_x(slot):
        h2b.send(part(slot, 192, 64, right), rf.at[0, slot, 64:128], XR)
        h2b.send(part(slot, 128, 64, left), rf.at[1, slot, 0:64], XL)

    def last_x(slot):
        sf[0, slot] = (part(slot, 128, 64, right)[...].astype(F32) + re[0, slot].astype(F32)).astype(BF16)
        h2b.send(sf.at[0, slot], rf.at[0, slot, 0:64], XR)
        sf[1, slot] = (part(slot, 192, 64, left)[...].astype(F32) + re[1, slot].astype(F32)).astype(BF16)
        h2b.send(sf.at[1, slot], rf.at[1, slot, 64:128], XL)

    h2early = first_x((ME, L, R))
    for slot in (ME, L, R):
        next_x(slot)

    for u, buf in ((0, xb), (1, cb)):
        @pl.loop(0, NZ, unroll=2)
        def _(k):
            gt[u, k] = nn(tr[u, :, 0:3 * TB], buf[0:3 * TB, cols(k, DZ)])

    orow = slice(OPP * TB, OPP * TB + TB)
    c3.wait()
    fcx["2"].wait()
    for h in range(2):
        s = slice(h * HB, (h + 1) * HB)
        acc[1, :, s] = nn(cb[orow], w[1, :, s])
    fxy.wait()
    for n, ax in enumerate((x, xl, xr)):
        lane = cols(ax, FX)
        term = nn(xb[orow, lane], w[0, lane, :])
        acc[0] = term if n == 0 else acc[0] + term
    fxy2.wait()
    pre = acc[0] + nn(xb[orow, far], w[0, far, :])
    finish(OPP, slice(0, 2 * HB), pre, acc[1])

    down = ([(0, 4), (1, 3), (0, 3), (1, 2), (0, 2), (1, 1), (0, 1)],
            [(1, 4), (0, 3), (1, 3), (0, 2), (1, 2), (0, 1), (1, 1)])
    todo = []
    for i in range(7):
        for way in range(2):
            u, k = down[way][i]
            todo.append((u, k if way == 0 else -k))
    todo += [(0, 0), (1, 0)]
    wsum = []

    def chunks(i):
        batch = Batch()
        for u, k in todo[2 * i:2 * i + 2]:
            az = step(z, k, NZ)
            value = gt[u, az] + nn(tr[u, :, 3 * TB:], (xb, cb)[u][orow, cols(az, DZ)])
            gs[u, az] = value[HB:].astype(BF16)
            batch.send(gs.at[u, az], pb.at[u, az], PC)
            gt[u, az, 0:HB] = value[:HB]
        wsum.append(batch)

    gz = []

    def total(u, k):
        az = step(z, k, NZ)
        return gt[u, az, 0:HB] + pb[u, az].astype(F32)

    def gsend(i):
        wsum[i].wait()
        if i >= 2:
            gz[i - 2].wait()
        batch = Batch()
        for way in range(2):
            u, k = down[way][i]
            value = total(u, k if way == 0 else -k)
            if i >= 2:
                value = value + rz[way, i - 2].astype(F32)
            sz[way, i] = value.astype(BF16)
            batch.send(sz.at[way, i], rz.at[way, i], (ZR, ZL)[way])
        gz.append(batch)

    chunks(0)
    chunks(1)
    gsend(0)
    partial(OPP, OPP + 1)
    h1 = []
    for r in (0, 32):
        h1.append(send(part(OPP, r, 32), ra.at[0, r:r + 32], YR)
                  .send(part(OPP, 64 + r, 32), ra.at[1, r:r + 32], YL))
    first_x((OPP,))
    next_x(OPP)
    gsend(1)
    h2early.wait()
    for slot in (ME, L, R):
        last_x(slot)
    chunks(2)
    gsend(2)
    chunks(3)
    chunks(4)
    def next_y(n, r):
        h1[n].wait()
        sb[0, r:r + 32] = (part(R, r, 32)[...].astype(F32) + ra[0, r:r + 32].astype(F32)).astype(BF16)
        h1b.send(sb.at[0, r:r + 32], rb.at[0, r:r + 32, :], YR)
        sb[1, r:r + 32] = (part(L, 64 + r, 32)[...].astype(F32) + ra[1, r:r + 32].astype(F32)).astype(BF16)
        h1b.send(sb.at[1, r:r + 32], rb.at[1, 64 + r:96 + r, :], YL)

    next_y(0, 0)
    gsend(3)
    h2[OPP].wait()
    last_x(OPP)
    next_y(1, 32)
    chunks(5)
    chunks(6)
    gsend(4)
    chunks(7)
    gsend(5)

    h2b.wait()
    here = cols(x, FX)
    for slot in range(4):
        q2[slot] = (part(slot, 128, 128, here)[...].astype(F32)
                    + rf[0, slot].astype(F32) + rf[1, slot].astype(F32))
    sh[0] = q2[OPP].astype(BF16)
    sh[1, 64:128] = q2[R, 64:128, :].astype(BF16)
    sh[2, 0:64] = q2[L, 0:64, :].astype(BF16)
    v2 = send(sh.at[0, 0:64, :], rg.at[0], YR).send(sh.at[0, 64:128, :], rg.at[1], YL)
    v2b = Batch()
    v2b.send(sh.at[1, 64:128, :], rh.at[0, 64:128, :], YR)
    v2b.send(sh.at[2, 0:64, :], rh.at[1, 0:64, :], YL)
    h1b.wait()
    for k in range(NX):
        s = slice(k * FX, (k + 1) * FX)
        q1[k] = g[0:128, s].astype(F32) + rb[0, :, s].astype(F32) + rb[1, :, s].astype(F32)
    sd[0] = q1[x2].astype(BF16)
    sd[1, 64:128] = q1[xr, 64:128, :].astype(BF16)
    sd[2, 0:64] = q1[xl, 0:64, :].astype(BF16)
    v1 = send(sd.at[0, 0:64, :], rc.at[0], XR).send(sd.at[0, 64:128, :], rc.at[1], XL)
    v1b = Batch()
    v1b.send(sd.at[1, 64:128, :], rd.at[0, 64:128, :], XR)
    v1b.send(sd.at[2, 0:64, :], rd.at[1, 0:64, :], XL)
    gsend(6)
    v2.wait()
    sh[1, 0:64] = (q2[R, 0:64, :] + rg[0].astype(F32)).astype(BF16)
    v2b.send(sh.at[1, 0:64, :], rh.at[0, 0:64, :], YR)
    sh[2, 64:128] = (q2[L, 64:128, :] + rg[1].astype(F32)).astype(BF16)
    v2b.send(sh.at[2, 64:128, :], rh.at[1, 64:128, :], YL)
    v1.wait()
    sd[1, 0:64] = (q1[xr, 0:64, :] + rc[0].astype(F32)).astype(BF16)
    v1b.send(sd.at[1, 0:64, :], rd.at[0, 0:64, :], XR)
    sd[2, 64:128] = (q1[xl, 64:128, :] + rc[1].astype(F32)).astype(BF16)
    v1b.send(sd.at[2, 64:128, :], rd.at[1, 64:128, :], XL)
    own, other = cols(c, 256), cols(o, 256)
    ends = Batch()
    stored = [0]

    def store(src, dst):
        pltpu.make_async_copy(src, dst, lsem.at[5]).start()
        stored[0] += size(src)

    def finish_rows(r, value, n):
        q1[n] = value
        fp[0, r:r + 128] = q1[n, :, other].astype(BF16)
        fp[1, r:r + 128] = q1[n, :, own].astype(BF16)
        row = pl.ds(pl.multiple_of(c * TB + r, 128), 128)
        ends.send(fp.at[0, r:r + 128], og.at[row, :], PC)
        store(fp.at[1, r:r + 128], og.at[row, :])

    v1b.wait()
    finish_rows(0, q1[x] + rd[0].astype(F32) + rd[1].astype(F32), 0)
    v2b.wait()
    finish_rows(128, q2[ME] + rh[0].astype(F32) + rh[1].astype(F32), 1)

    scale = 1.0 / 128.0
    ops = Batch()
    wsum[7].wait()
    gz[5].wait()
    gz[6].wait()
    for u in range(2):
        value = total(u, 0) + rz[0, 6 - u].astype(F32) + rz[1, 5 + u].astype(F32)
        fs_s[u] = (value * scale).T.astype(BF16)
        there = cols(y, HB)
        for ay, where in ((y2, Y2), (yr, YR), (yl, YL)):
            ops.send(fs_s.at[u, cols(ay, RY), :], ow.at[u, :, there], where, small=True)
        store(fs_s.at[u, cols(y, RY), :], ow.at[u, :, there])
    ops.wait()
    ends.wait()
    ref = span(stored[0])
    pltpu.make_async_copy(ref, ref, lsem.at[5]).wait()
    for k, (n, _) in enumerate(groups):
        ref = span(n)
        pltpu.make_async_copy(ref, ref, ssem.at[k]).wait()


def finisher(ow, og, ig_out, ug_out, dg_out, wv, gv, fv, sem):
    loads = [pltpu.make_async_copy(ow.at[u], wv.at[u], sem.at[u]) for u in range(2)]
    loads.append(pltpu.make_async_copy(og, gv, sem.at[2]))
    for copy in loads:
        copy.start()
    stores = []
    for u, out in ((0, ug_out), (1, dg_out)):
        loads[u].wait()
        fv[u] = wv[u].astype(F32)
        stores.append(pltpu.make_async_copy(fv.at[u], out, sem.at[3 + u]))
        stores[-1].start()
    loads[2].wait()
    stores.append(pltpu.make_async_copy(gv, ig_out, sem.at[5]))
    stores[-1].start()
    for copy in stores:
        copy.wait()


def per_device(normed_input, cotangent, up_weight, down_weight):
    bf = lambda *s: pltpu.VMEM(s, BF16)
    f4 = lambda *s: pltpu.VMEM(s, F32)
    hbm = pl.BlockSpec(memory_space=pl.ANY)
    shape = jax.ShapeDtypeStruct
    ow, og = pl.pallas_call(
        kernel,
        out_shape=(shape((2, RY, 4 * HB), BF16), shape((2 * TB, 256), BF16)),
        in_specs=[hbm] * 4,
        out_specs=(hbm,) * 2,
        scratch_shapes=[
            bf(NY * TB, D), bf(NY * TB, D),
            bf(2, D, 2 * HB),
            bf(TB, 256), bf(TB, 256),
            bf(2, RY, 4 * HB),
            bf(NY * TB, 2 * HB),
            bf(2, 2 * HB, NY * TB),
            f4(2, TB, 2 * HB),
            f4(2, NZ, 2 * HB, DZ),
            bf(2, NZ, HB, DZ), bf(2, NZ, HB, DZ),
            bf(2, 7, HB, DZ), bf(2, 7, HB, DZ),
            bf(2, DZ, HB),
            bf(NY * TB, D),
            bf(2, 64, D), bf(2, 128, D), bf(2, 64, D),
            f4(NX, 128, FX),
            bf(2, 64, FX), bf(2, 128, FX), bf(3, 128, FX),
            bf(2, NY, 64, FX), bf(2, NY, 128, FX), bf(2, NY, 64, FX),
            f4(NY, 128, FX),
            bf(2, 64, FX), bf(2, 128, FX), bf(3, 128, FX),
            bf(2, TB, 256),
            pltpu.SemaphoreType.DMA((6,)),
            pltpu.SemaphoreType.DMA((SENDS,)),
            pltpu.SemaphoreType.DMA((RECVS,)),
        ],
        compiler_params=pltpu.CompilerParams(
            collective_id=0, has_side_effects=True, vmem_limit_bytes=60 * 1024 * 1024
        ),
    )(normed_input, cotangent, up_weight, down_weight.T)
    ig, ug, dg = pl.pallas_call(
        finisher,
        out_shape=(shape((2 * TB, 256), BF16), shape((RY, 4 * HB), F32), shape((RY, 4 * HB), F32)),
        in_specs=[hbm] * 2,
        out_specs=(hbm,) * 3,
        scratch_shapes=[
            bf(2, RY, 4 * HB), bf(2 * TB, 256), f4(2, RY, 4 * HB), pltpu.SemaphoreType.DMA((6,)),
        ],
    )(ow, og)
    return ig, ug, dg.T


def solution(mesh):
    return jax.shard_map(
        per_device, mesh=mesh,
        in_specs=(P("fs", "tp"), P("fs", "tp"), P("fs", "tp"), P("tp", "fs")),
        out_specs=(P("fs", "tp"), P("fs", "tp"), P("tp", "fs")),
        check_vma=False,
    )
```

```python
import math

import jax
import jax.numpy as jnp
from jax import lax
from jax.experimental import pallas as pl
from jax.experimental.pallas import tpu as pltpu
from jax.sharding import PartitionSpec as P

NX, NY, NZ = 4, 4, 8
D = 2048
TB = 256
FX = 512
HB = 256
DZ = 256
RY = 64
HALF = TB // 2
CUT = 112
MID = (96, 160)
SENDS, RECVS = 6, 61
MESH = pl.DeviceIdType.MESH
BF16, F32 = jnp.bfloat16, jnp.float32


def nn(a, b):
    return lax.dot_general(a, b, (((1,), (0,)), ((), ())), preferred_element_type=F32)


def nt(a, b):
    return lax.dot_general(a, b, (((1,), (1,)), ((), ())), preferred_element_type=F32)


def kernel(
    x_in, c_in, up_in, dn_in, ow, og,
    xb, cb, w, xs, cs, uv, pg, tr, acc, gp, gt, gs, pb, rz, sz, fs_s, g,
    ra, rb, sb, q1, rc, rd, sd, re, rf, sf, q2, rg, rh, sh, fp,
    lsem, ssem, rsem,
):
    fs, tp = lax.axis_index("fs"), lax.axis_index("tp")
    z, y = lax.div(fs, NY), lax.rem(fs, NY)
    x, c = lax.div(tp, 2), lax.rem(tp, 2)
    o = 1 - c
    step = lambda a, k, n: lax.rem(a + (k % n), n)
    xr, xl, x2 = step(x, 1, NX), step(x, -1, NX), step(x, 2, NX)
    yr, yl, y2 = step(y, 1, NY), step(y, -1, NY), step(y, 2, NY)
    at = lambda ax, ay, az, ac: (az * NY + ay, ax * 2 + ac)
    XR, XL = at(xr, y, z, c), at(xl, y, z, c)
    YR, YL, Y2 = at(x, yr, z, c), at(x, yl, z, c), at(x, y2, z, c)
    ZR, ZL = at(x, y, step(z, 1, NZ), c), at(x, y, step(z, -1, NZ), c)
    PC = at(x, y, z, o)
    ME, L, R, OPP = range(4)

    arrivals = iter(range(RECVS))
    groups = []
    SPAN = 4 << 20

    def size(ref):
        return math.prod(ref.shape) * 2

    def span(count):
        return xb.at[0:count // (2 * D), :]

    class Batch:
        def __init__(self):
            self.sem, self.bytes = rsem.at[next(arrivals)], 0

        def send(self, src, dst, where, small=False):
            n = size(src)
            at = next((k for k, g in enumerate(groups) if g[1] == small and g[0] + n <= SPAN), None)
            if at is None:
                at = len(groups)
                groups.append([0, small])
            groups[at][0] += n
            self.bytes += n
            pltpu.make_async_remote_copy(
                src_ref=src, dst_ref=dst, send_sem=ssem.at[at], recv_sem=self.sem,
                device_id=where, device_id_type=MESH,
            ).start()
            return self

        def wait(self):
            ref = span(self.bytes)
            pltpu.make_async_copy(ref, ref, self.sem).wait()

    def send(src, dst, where):
        return Batch().send(src, dst, where)

    def cols(k, n):
        return pl.ds(pl.multiple_of(k * n, n), n)

    mine = pl.ds(pl.multiple_of(x * FX + c * 256, 256), 256)
    wrow = pl.ds(pl.multiple_of(z * DZ + y * RY, RY), RY)
    loads = []
    for i, pairs in enumerate((
        ((c_in.at[cols(o, TB), :], cs),),
        ((x_in.at[cols(o, TB), :], xs),),
        ((up_in, uv.at[0]), (dn_in, uv.at[1])),
        ((c_in.at[cols(c, TB), :], cb.at[0:TB, mine]), (x_in.at[cols(c, TB), :], xb.at[0:TB, mine])),
        ((up_in.at[:, cols(y, HB)], w.at[0, wrow, 0:HB]),
         (dn_in.at[:, cols(y, HB)], w.at[1, wrow, 0:HB])),
    )):
        for src, dst in pairs:
            pltpu.make_async_copy(src, dst, lsem.at[i]).start()
        ref = span(sum(size(dst) for _, dst in pairs))
        loads.append(pltpu.make_async_copy(ref, ref, lsem.at[i]))

    barrier = pltpu.get_barrier_semaphore()
    peers = (XR, XL, YR, YL, Y2, ZR, ZL, PC)
    for peer in peers:
        pl.semaphore_signal(barrier, inc=1, device_id=peer, device_id_type=MESH)
    pl.semaphore_wait(barrier, len(peers))

    loads[0].wait()
    cop = send(cs, cb.at[0:TB, mine], PC)
    loads[1].wait()
    xop = send(xs, xb.at[0:TB, mine], PC)
    loads[2].wait()
    loads[3].wait()
    x_x = Batch()
    for way in (XR, XL):
        x_x.send(xb.at[0:TB, mine], xb.at[0:TB, mine], way)
    wops = Batch()
    for ay, where in ((y2, Y2), (yr, YR), (yl, YL)):
        for u in range(2):
            wops.send(uv.at[u, :, cols(ay, HB)], w.at[u, wrow, 0:HB], where, small=True)

    def blk(buf, slot, ax, lo=0, hi=TB):
        return buf.at[slot * TB + lo:slot * TB + hi, cols(ax, FX)]

    def over_x(buf, slot, ax):
        ref = blk(buf, slot, ax)
        return send(ref, ref, XR).send(ref, ref, XL)

    def over_y(buf, ax):
        ref = blk(buf, ME, ax)
        return send(ref, blk(buf, L, ax), YR).send(ref, blk(buf, R, ax), YL)

    def pass_x(buf, slot, batch):
        batch.wait()
        a, b = blk(buf, slot, xl, 0, HALF), blk(buf, slot, xr, HALF)
        return send(a, a, XR).send(b, b, XL)

    def pass_y(buf, ax, batch, out=None, lo=CUT, hi=CUT):
        batch.wait()
        out = out or Batch()
        out.send(blk(buf, L, ax, 0, lo), blk(buf, OPP, ax, 0, lo), YR)
        return out.send(blk(buf, R, ax, hi), blk(buf, OPP, ax, hi), YL)

    cop.wait()
    c_y = over_y(cb, x)
    there = pl.ds(pl.multiple_of(x * FX + o * 256, 256), 256)
    xop.wait()
    for way in (XR, XL):
        x_x.send(xb.at[0:TB, there], xb.at[0:TB, there], way)
    x_y = {"me": over_y(xb, x)}
    c_x = {"me": over_x(cb, ME, x)}

    loads[4].wait()
    wops.wait()

    wz = []
    wpc = Batch()
    order = ([(0, 0), (1, 0), (0, 1), (1, 1), (0, 2), (1, 2), (0, 3)],
             [(1, 0), (0, 0), (1, 1), (0, 1), (1, 2), (0, 2), (1, 3)])

    def wsend(i):
        batch = Batch()
        for way in range(2):
            u, k = order[way][i]
            ref = w.at[u, cols(step(z, -k if way == 0 else k, NZ), DZ), 0:HB]
            batch.send(ref, ref, (ZR, ZL)[way])
        wz.append(batch)

    def wpair(u, k):
        rows = cols(step(z, k, NZ), DZ)
        wpc.send(w.at[u, rows, 0:HB], w.at[u, rows, HB:2 * HB], PC)

    wsend(0)
    wsend(1)
    for u in range(2):
        wpair(u, 0)

    def warrive(i):
        wz[i].wait()
        if i + 2 < 7:
            wsend(i + 2)
        for way in range(2):
            u, k = order[way][i]
            wpair(u, -(k + 1) if way == 0 else k + 1)

    fx = pass_x(xb, ME, x_x)
    warrive(0)
    fc = pass_y(cb, x, c_y)
    x_y["l"] = over_y(xb, xl)
    x_y["r"] = over_y(xb, xr)
    warrive(1)
    fcx = {"me": pass_x(cb, ME, c_x["me"])}
    c_x["l"] = over_x(cb, L, x)
    c_x["r"] = over_x(cb, R, x)
    warrive(2)
    fx.wait()
    x_y["2"] = over_y(xb, x2)
    warrive(3)
    fxym = pass_y(xb, x, x_y["me"])
    fc.wait()
    warrive(4)
    warrive(5)
    fcx["l"] = pass_x(cb, L, c_x["l"])
    fxy = pass_y(xb, xl, x_y["l"], None, *MID)
    warrive(6)
    fcx["me"].wait()
    wpc.wait()

    def forward(slot):
        rows = slice(slot * TB, (slot + 1) * TB)
        for h in range(2):
            s = slice(h * HB, (h + 1) * HB)
            pre = nn(xb[rows], w[0, :, s])
            act_grad = nn(cb[rows], w[1, :, s])
            finish(slot, s, pre, act_grad)

    def finish(slot, s, pre, act_grad):
        rows = slice(slot * TB, (slot + 1) * TB)
        rect = jnp.maximum(pre, 0.0)
        grad = 2.0 * rect * act_grad
        pg[rows, s] = grad.astype(BF16)
        tr[0, s, rows] = grad.T.astype(BF16)
        tr[1, s, rows] = (rect * rect).T.astype(BF16)

    def partial(lo, hi):
        rows = slice(lo * TB, hi * TB)

        @pl.loop(0, NZ, unroll=2)
        def _(k):
            lane = cols(k, DZ)
            g[rows, lane] = nt(pg[rows, :], w[0, lane, :]).astype(BF16)

    forward(ME)
    fcx["r"] = pass_x(cb, R, c_x["r"])
    lo, hi = blk(cb, OPP, x, 0, HALF), blk(cb, OPP, x, HALF)
    c2 = send(lo, lo, XR).send(hi, hi, XL)
    c3 = send(hi, hi, XR).send(lo, lo, XL)
    partial(ME, L)
    pass_y(xb, xr, x_y["r"], fxy, *MID)
    fxy2 = pass_y(xb, x2, x_y["2"])
    fcx["l"].wait()
    forward(L)
    fcx["r"].wait()
    forward(R)
    fcx["2"] = pass_x(cb, OPP, c2)
    partial(L, OPP)
    fxym.wait()
    mid = blk(xb, OPP, x, *MID)
    fmid = send(mid, mid, XR).send(mid, mid, XL)

    def part(slot, r, n, lane=slice(None)):
        return g.at[slot * TB + r:slot * TB + r + n, lane]

    h1b = Batch()
    h1b.send(part(R, 64, 64), rb.at[0, 64:128, :], YR)
    h1b.send(part(L, 0, 64), rb.at[1, 0:64, :], YL)
    far, right, left = cols(x2, FX), cols(xr, FX), cols(xl, FX)
    h2, h2b = {}, Batch()

    def first_x(slots):
        batch = Batch()
        for slot in slots:
            batch.send(part(slot, 128, 64, far), re.at[0, slot], XR)
            batch.send(part(slot, 192, 64, far), re.at[1, slot], XL)
            h2[slot] = batch
        return batch

    def next_x(slot):
        h2b.send(part(slot, 192, 64, right), rf.at[0, slot, 64:128], XR)
        h2b.send(part(slot, 128, 64, left), rf.at[1, slot, 0:64], XL)

    def last_x(slot):
        sf[0, slot] = (part(slot, 128, 64, right)[...].astype(F32) + re[0, slot].astype(F32)).astype(BF16)
        h2b.send(sf.at[0, slot], rf.at[0, slot, 0:64], XR)
        sf[1, slot] = (part(slot, 192, 64, left)[...].astype(F32) + re[1, slot].astype(F32)).astype(BF16)
        h2b.send(sf.at[1, slot], rf.at[1, slot, 64:128], XL)

    h2early = first_x((ME, L, R))
    for slot in (ME, L, R):
        next_x(slot)

    down = ([(0, 4), (1, 3), (0, 3), (1, 2), (0, 2), (1, 1), (0, 1)],
            [(1, 4), (0, 3), (1, 3), (0, 2), (1, 2), (0, 1), (1, 1)])
    todo = []
    for i in range(7):
        for way in range(2):
            u, k = down[way][i]
            todo.append((u, k if way == 0 else -k))
    todo += [(0, 0), (1, 0)]
    wsum = []

    def term(n, rows, lo, hi):
        u, k = todo[n]
        return nn(tr[u, rows, lo * TB:hi * TB], (xb, cb)[u][lo * TB:hi * TB, cols(step(z, k, NZ), DZ)])

    def early(*which):
        for n in which:
            gp[n] = term(n, slice(None), 0, 3)

    def give(batch, n, value):
        u, k = todo[n]
        az = step(z, k, NZ)
        gs[u, az] = value.astype(BF16)
        batch.send(gs.at[u, az], pb.at[u, az], PC)

    def keep(n, value):
        u, k = todo[n]
        gt[u, step(z, k, NZ)] = value

    def chunks(i, split=False):
        batch = Batch()
        pair = (2 * i, 2 * i + 1)
        if split:
            for n in pair:
                give(batch, n, gp[n, HB:] + term(n, slice(HB, 2 * HB), 3, 4))
            for n in pair:
                keep(n, gp[n, :HB] + term(n, slice(0, HB), 3, 4))
        else:
            for n in pair:
                value = gp[n] + term(n, slice(None), 3, 4)
                give(batch, n, value[HB:])
                keep(n, value[:HB])
        wsum.append(batch)

    early(*range(14))

    orow = slice(OPP * TB, OPP * TB + TB)
    c3.wait()
    fcx["2"].wait()
    for h in range(2):
        s = slice(h * HB, (h + 1) * HB)
        acc[1, :, s] = nn(cb[orow], w[1, :, s])
    early(14, 15)
    fxy.wait()
    fmid.wait()
    for n, ax in enumerate((x, xl, xr)):
        lane = cols(ax, FX)
        more = nn(xb[orow, lane], w[0, lane, :])
        acc[0] = more if n == 0 else acc[0] + more
    fxy2.wait()
    pre = acc[0] + nn(xb[orow, far], w[0, far, :])
    finish(OPP, slice(0, 2 * HB), pre, acc[1])

    gz = []

    def total(u, k):
        az = step(z, k, NZ)
        return gt[u, az] + pb[u, az].astype(F32)

    def gsend(i):
        wsum[i].wait()
        if i >= 2:
            gz[i - 2].wait()
        batch = Batch()
        for way in range(2):
            u, k = down[way][i]
            value = total(u, k if way == 0 else -k)
            if i >= 2:
                value = value + rz[way, i - 2].astype(F32)
            sz[way, i] = value.astype(BF16)
            if i < 6:
                batch.send(sz.at[way, i], rz.at[way, i], (ZR, ZL)[way])
        gz.append(batch)
        if i == 6:
            for rows in (slice(0, 128), slice(128, 256)):
                batch = Batch()
                for way in range(2):
                    batch.send(sz.at[way, i, rows], rz.at[way, i, rows], (ZR, ZL)[way])
                gz.append(batch)

    chunks(0, split=True)
    chunks(1)
    gsend(0)
    partial(OPP, OPP + 1)
    h1 = []
    for r in (0, 32):
        h1.append(send(part(OPP, r, 32), ra.at[0, r:r + 32], YR)
                  .send(part(OPP, 64 + r, 32), ra.at[1, r:r + 32], YL))
    first_x((OPP,))
    next_x(OPP)
    gsend(1)
    h2early.wait()
    for slot in (ME, L, R):
        last_x(slot)
    chunks(2)
    gsend(2)
    chunks(3)
    def next_y(n, r):
        h1[n].wait()
        sb[0, r:r + 32] = (part(R, r, 32)[...].astype(F32) + ra[0, r:r + 32].astype(F32)).astype(BF16)
        h1b.send(sb.at[0, r:r + 32], rb.at[0, r:r + 32, :], YR)
        sb[1, r:r + 32] = (part(L, 64 + r, 32)[...].astype(F32) + ra[1, r:r + 32].astype(F32)).astype(BF16)
        h1b.send(sb.at[1, r:r + 32], rb.at[1, 64 + r:96 + r, :], YL)

    next_y(0, 0)
    gsend(3)
    h2[OPP].wait()
    last_x(OPP)
    next_y(1, 32)
    chunks(4)
    gsend(4)
    chunks(5)

    h2b.wait()
    here = cols(x, FX)
    for slot in range(4):
        q2[slot] = (part(slot, 128, 128, here)[...].astype(F32)
                    + rf[0, slot].astype(F32) + rf[1, slot].astype(F32))
    sh[0] = q2[OPP].astype(BF16)
    sh[1, 64:128] = q2[R, 64:128, :].astype(BF16)
    sh[2, 0:64] = q2[L, 0:64, :].astype(BF16)
    v2 = send(sh.at[0, 0:64, :], rg.at[0], YR).send(sh.at[0, 64:128, :], rg.at[1], YL)
    v2b = Batch()
    v2b.send(sh.at[1, 64:128, :], rh.at[0, 64:128, :], YR)
    v2b.send(sh.at[2, 0:64, :], rh.at[1, 0:64, :], YL)
    gsend(5)
    h1b.wait()
    for k in range(NX):
        s = slice(k * FX, (k + 1) * FX)
        q1[k] = g[0:128, s].astype(F32) + rb[0, :, s].astype(F32) + rb[1, :, s].astype(F32)
    sd[0] = q1[x2].astype(BF16)
    sd[1, 64:128] = q1[xr, 64:128, :].astype(BF16)
    sd[2, 0:64] = q1[xl, 0:64, :].astype(BF16)
    v1 = send(sd.at[0, 0:64, :], rc.at[0], XR).send(sd.at[0, 64:128, :], rc.at[1], XL)
    v1b = Batch()
    v1b.send(sd.at[1, 64:128, :], rd.at[0, 64:128, :], XR)
    v1b.send(sd.at[2, 0:64, :], rd.at[1, 0:64, :], XL)
    chunks(6)
    chunks(7)
    v2.wait()
    sh[1, 0:64] = (q2[R, 0:64, :] + rg[0].astype(F32)).astype(BF16)
    v2b.send(sh.at[1, 0:64, :], rh.at[0, 0:64, :], YR)
    sh[2, 64:128] = (q2[L, 64:128, :] + rg[1].astype(F32)).astype(BF16)
    v2b.send(sh.at[2, 64:128, :], rh.at[1, 64:128, :], YL)
    gsend(6)
    v1.wait()
    sd[1, 0:64] = (q1[xr, 0:64, :] + rc[0].astype(F32)).astype(BF16)
    v1b.send(sd.at[1, 0:64, :], rd.at[0, 0:64, :], XR)
    sd[2, 64:128] = (q1[xl, 64:128, :] + rc[1].astype(F32)).astype(BF16)
    v1b.send(sd.at[2, 64:128, :], rd.at[1, 64:128, :], XL)
    own, other = cols(c, 256), cols(o, 256)
    ends = Batch()
    stored = [0]

    def store(src, dst):
        pltpu.make_async_copy(src, dst, lsem.at[5]).start()
        stored[0] += size(src)

    def finish_rows(r, value, n):
        q1[n] = value
        fp[0, r:r + 128] = q1[n, :, other].astype(BF16)
        fp[1, r:r + 128] = q1[n, :, own].astype(BF16)
        row = pl.ds(pl.multiple_of(c * TB + r, 128), 128)
        ends.send(fp.at[0, r:r + 128], og.at[row, :], PC)
        store(fp.at[1, r:r + 128], og.at[row, :])

    scale = 1.0 / 128.0
    ops = Batch()
    wsum[7].wait()
    gz[5].wait()
    for half in range(2):
        gz[7 + half].wait()
        rows = slice(half * 128, half * 128 + 128)
        lane = pl.ds(pl.multiple_of(y * HB + half * 128, 128), 128)
        for u in range(2):
            value = gt[u, z, rows] + pb[u, z, rows].astype(F32)
            value = value + rz[0, 6 - u, rows].astype(F32) + rz[1, 5 + u, rows].astype(F32)
            fs_s[u, half] = (value * scale).T.astype(BF16)
            for ay, where in ((y2, Y2), (yr, YR), (yl, YL)):
                ops.send(fs_s.at[u, half, cols(ay, RY), :], ow.at[u, :, lane], where, small=True)
            store(fs_s.at[u, half, cols(y, RY), :], ow.at[u, :, lane])

    v1b.wait()
    finish_rows(0, q1[x] + rd[0].astype(F32) + rd[1].astype(F32), 0)
    v2b.wait()
    finish_rows(128, q2[ME] + rh[0].astype(F32) + rh[1].astype(F32), 1)

    ops.wait()
    ends.wait()
    ref = span(stored[0])
    pltpu.make_async_copy(ref, ref, lsem.at[5]).wait()
    for k, (n, _) in enumerate(groups):
        ref = span(n)
        pltpu.make_async_copy(ref, ref, ssem.at[k]).wait()


def finisher(ow, og, ig_out, ug_out, dg_out, wv, gv, fv, sem):
    loads = [pltpu.make_async_copy(ow.at[u], wv.at[u], sem.at[u]) for u in range(2)]
    loads.append(pltpu.make_async_copy(og, gv, sem.at[2]))
    for copy in loads:
        copy.start()
    stores = []
    for u, out in ((0, ug_out), (1, dg_out)):
        loads[u].wait()
        fv[u] = wv[u].astype(F32)
        stores.append(pltpu.make_async_copy(fv.at[u], out, sem.at[3 + u]))
        stores[-1].start()
    loads[2].wait()
    stores.append(pltpu.make_async_copy(gv, ig_out, sem.at[5]))
    stores[-1].start()
    for copy in stores:
        copy.wait()


def per_device(normed_input, cotangent, up_weight, down_weight):
    bf = lambda *s: pltpu.VMEM(s, BF16)
    f4 = lambda *s: pltpu.VMEM(s, F32)
    hbm = pl.BlockSpec(memory_space=pl.ANY)
    shape = jax.ShapeDtypeStruct
    ow, og = pl.pallas_call(
        kernel,
        out_shape=(shape((2, RY, 4 * HB), BF16), shape((2 * TB, 256), BF16)),
        in_specs=[hbm] * 4,
        out_specs=(hbm,) * 2,
        scratch_shapes=[
            bf(NY * TB, D), bf(NY * TB, D),
            bf(2, D, 2 * HB),
            bf(TB, 256), bf(TB, 256),
            bf(2, RY, 4 * HB),
            bf(NY * TB, 2 * HB),
            bf(2, 2 * HB, NY * TB),
            f4(2, TB, 2 * HB),
            f4(2 * NZ, 2 * HB, DZ),
            f4(2, NZ, HB, DZ),
            bf(2, NZ, HB, DZ), bf(2, NZ, HB, DZ),
            bf(2, 7, HB, DZ), bf(2, 7, HB, DZ),
            bf(2, 2, DZ, 128),
            bf(NY * TB, D),
            bf(2, 64, D), bf(2, 128, D), bf(2, 64, D),
            f4(NX, 128, FX),
            bf(2, 64, FX), bf(2, 128, FX), bf(3, 128, FX),
            bf(2, NY, 64, FX), bf(2, NY, 128, FX), bf(2, NY, 64, FX),
            f4(NY, 128, FX),
            bf(2, 64, FX), bf(2, 128, FX), bf(3, 128, FX),
            bf(2, TB, 256),
            pltpu.SemaphoreType.DMA((6,)),
            pltpu.SemaphoreType.DMA((SENDS,)),
            pltpu.SemaphoreType.DMA((RECVS,)),
        ],
        compiler_params=pltpu.CompilerParams(
            collective_id=0, has_side_effects=True, vmem_limit_bytes=60 * 1024 * 1024
        ),
    )(normed_input, cotangent, up_weight, down_weight.T)
    ig, ug, dg = pl.pallas_call(
        finisher,
        out_shape=(shape((2 * TB, 256), BF16), shape((RY, 4 * HB), F32), shape((RY, 4 * HB), F32)),
        in_specs=[hbm] * 2,
        out_specs=(hbm,) * 3,
        scratch_shapes=[
            bf(2, RY, 4 * HB), bf(2 * TB, 256), f4(2, RY, 4 * HB), pltpu.SemaphoreType.DMA((6,)),
        ],
    )(ow, og)
    return ig, ug, dg.T


def solution(mesh):
    return jax.shard_map(
        per_device, mesh=mesh,
        in_specs=(P("fs", "tp"), P("fs", "tp"), P("fs", "tp"), P("tp", "fs")),
        out_specs=(P("fs", "tp"), P("fs", "tp"), P("tp", "fs")),
        check_vma=False,
    )
```

```python
import math

import jax
import jax.numpy as jnp
from jax import lax
from jax.experimental import pallas as pl
from jax.experimental.pallas import tpu as pltpu
from jax.sharding import PartitionSpec as P

NX, NY, NZ = 4, 4, 8
D = 2048
TB = 256
FX = 512
HB = 256
DZ = 256
RY = 64
HALF = TB // 2
CUT = 112
MID = (96, 160)
SENDS, RECVS = 6, 66
MESH = pl.DeviceIdType.MESH
BF16, F32 = jnp.bfloat16, jnp.float32


def nn(a, b):
    return lax.dot_general(a, b, (((1,), (0,)), ((), ())), preferred_element_type=F32)


def nt(a, b):
    return lax.dot_general(a, b, (((1,), (1,)), ((), ())), preferred_element_type=F32)


def kernel(
    x_in, c_in, up_in, dn_in, ow, og,
    xb, cb, w, xs, cs, uv, pg, tr, acc, gp, gt, gs, pb, rz, sz, fs_s, g,
    ra, rb, sb, q1, rc, rd, sd, re, rf, sf, q2, rg, rh, sh, fp,
    lsem, ssem, rsem,
):
    fs, tp = lax.axis_index("fs"), lax.axis_index("tp")
    z, y = lax.div(fs, NY), lax.rem(fs, NY)
    x, c = lax.div(tp, 2), lax.rem(tp, 2)
    o = 1 - c
    step = lambda a, k, n: lax.rem(a + (k % n), n)
    xr, xl, x2 = step(x, 1, NX), step(x, -1, NX), step(x, 2, NX)
    yr, yl, y2 = step(y, 1, NY), step(y, -1, NY), step(y, 2, NY)
    at = lambda ax, ay, az, ac: (az * NY + ay, ax * 2 + ac)
    XR, XL = at(xr, y, z, c), at(xl, y, z, c)
    YR, YL, Y2 = at(x, yr, z, c), at(x, yl, z, c), at(x, y2, z, c)
    ZR, ZL = at(x, y, step(z, 1, NZ), c), at(x, y, step(z, -1, NZ), c)
    PC = at(x, y, z, o)
    mate = y + 1 - 2 * lax.rem(y, 2)
    MATE, ACROSS = at(x, mate, z, c), at(x, step(mate, 2, NY), z, c)
    ME, L, R, OPP = range(4)

    arrivals = iter(range(RECVS))
    groups = []
    SPAN = 4 << 20

    def size(ref):
        return math.prod(ref.shape) * 2

    def span(count):
        return xb.at[0:count // (2 * D), :]

    class Batch:
        def __init__(self):
            self.sem, self.bytes = rsem.at[next(arrivals)], 0

        def send(self, src, dst, where, small=False):
            n = size(src)
            at = next((k for k, g in enumerate(groups) if g[1] == small and g[0] + n <= SPAN), None)
            if at is None:
                at = len(groups)
                groups.append([0, small])
            groups[at][0] += n
            self.bytes += n
            pltpu.make_async_remote_copy(
                src_ref=src, dst_ref=dst, send_sem=ssem.at[at], recv_sem=self.sem,
                device_id=where, device_id_type=MESH,
            ).start()
            return self

        def wait(self):
            ref = span(self.bytes)
            pltpu.make_async_copy(ref, ref, self.sem).wait()

    def send(src, dst, where):
        return Batch().send(src, dst, where)

    def cols(k, n):
        return pl.ds(pl.multiple_of(k * n, n), n)

    mine = pl.ds(pl.multiple_of(x * FX + c * 256, 256), 256)
    wrow = pl.ds(pl.multiple_of(z * DZ + y * RY, RY), RY)
    loads = []
    for i, pairs in enumerate((
        ((c_in.at[cols(o, TB), :], cs),),
        ((x_in.at[cols(o, TB), :], xs),),
        ((up_in, uv.at[0]), (dn_in, uv.at[1])),
        ((c_in.at[cols(c, TB), :], cb.at[0:TB, mine]), (x_in.at[cols(c, TB), :], xb.at[0:TB, mine])),
        ((up_in.at[:, cols(y, HB)], w.at[0, wrow, 0:HB]),
         (dn_in.at[:, cols(y, HB)], w.at[1, wrow, 0:HB])),
    )):
        for src, dst in pairs:
            pltpu.make_async_copy(src, dst, lsem.at[i]).start()
        ref = span(sum(size(dst) for _, dst in pairs))
        loads.append(pltpu.make_async_copy(ref, ref, lsem.at[i]))

    barrier = pltpu.get_barrier_semaphore()
    peers = (XR, XL, YR, YL, Y2, ZR, ZL, PC)
    for peer in peers:
        pl.semaphore_signal(barrier, inc=1, device_id=peer, device_id_type=MESH)
    pl.semaphore_wait(barrier, len(peers))

    loads[0].wait()
    cop = send(cs, cb.at[0:TB, mine], PC)
    loads[1].wait()
    xop = send(xs, xb.at[0:TB, mine], PC)
    loads[2].wait()
    loads[3].wait()
    x_x = Batch()
    for way in (XR, XL):
        x_x.send(xb.at[0:TB, mine], xb.at[0:TB, mine], way)
    wops = Batch()
    for ay, where in ((y2, Y2), (yr, YR), (yl, YL)):
        for u in range(2):
            wops.send(uv.at[u, :, cols(ay, HB)], w.at[u, wrow, 0:HB], where, small=True)

    def blk(buf, slot, ax, lo=0, hi=TB):
        return buf.at[slot * TB + lo:slot * TB + hi, cols(ax, FX)]

    def over_x(buf, slot, ax):
        ref = blk(buf, slot, ax)
        return send(ref, ref, XR).send(ref, ref, XL)

    def over_y(buf, ax):
        ref = blk(buf, ME, ax)
        return send(ref, blk(buf, L, ax), YR).send(ref, blk(buf, R, ax), YL)

    def pass_x(buf, slot, batch):
        batch.wait()
        a, b = blk(buf, slot, xl, 0, HALF), blk(buf, slot, xr, HALF)
        return send(a, a, XR).send(b, b, XL)

    def pass_y(buf, ax, batch, out=None, lo=CUT, hi=CUT):
        batch.wait()
        out = out or Batch()
        out.send(blk(buf, L, ax, 0, lo), blk(buf, OPP, ax, 0, lo), YR)
        return out.send(blk(buf, R, ax, hi), blk(buf, OPP, ax, hi), YL)

    cop.wait()
    c_y = over_y(cb, x)
    there = pl.ds(pl.multiple_of(x * FX + o * 256, 256), 256)
    xop.wait()
    for way in (XR, XL):
        x_x.send(xb.at[0:TB, there], xb.at[0:TB, there], way)
    x_y = {"me": over_y(xb, x)}
    c_x = {"me": over_x(cb, ME, x)}

    loads[4].wait()
    wops.wait()

    wz = []
    wpc = Batch()
    order = ([(0, 0), (1, 0), (0, 1), (1, 1), (0, 2), (1, 2), (0, 3)],
             [(1, 0), (0, 0), (1, 1), (0, 1), (1, 2), (0, 2), (1, 3)])

    def wsend(i):
        batch = Batch()
        for way in range(2):
            u, k = order[way][i]
            ref = w.at[u, cols(step(z, -k if way == 0 else k, NZ), DZ), 0:HB]
            batch.send(ref, ref, (ZR, ZL)[way])
        wz.append(batch)

    def wpair(u, k):
        rows = cols(step(z, k, NZ), DZ)
        wpc.send(w.at[u, rows, 0:HB], w.at[u, rows, HB:2 * HB], PC)

    wsend(0)
    wsend(1)
    for u in range(2):
        wpair(u, 0)

    def warrive(i):
        wz[i].wait()
        if i + 2 < 7:
            wsend(i + 2)
        for way in range(2):
            u, k = order[way][i]
            wpair(u, -(k + 1) if way == 0 else k + 1)

    fx = pass_x(xb, ME, x_x)
    warrive(0)
    fc = pass_y(cb, x, c_y)
    x_y["l"] = over_y(xb, xl)
    x_y["r"] = over_y(xb, xr)
    warrive(1)
    fcx = {"me": pass_x(cb, ME, c_x["me"])}
    c_x["l"] = over_x(cb, L, x)
    c_x["r"] = over_x(cb, R, x)
    warrive(2)
    fx.wait()
    x_y["2"] = over_y(xb, x2)
    warrive(3)
    fxym = pass_y(xb, x, x_y["me"])
    fc.wait()
    warrive(4)
    warrive(5)
    fcx["l"] = pass_x(cb, L, c_x["l"])
    fxy = pass_y(xb, xl, x_y["l"], None, *MID)
    warrive(6)
    fcx["me"].wait()
    wpc.wait()

    def forward(slot):
        rows = slice(slot * TB, (slot + 1) * TB)
        for h in range(2):
            s = slice(h * HB, (h + 1) * HB)
            pre = nn(xb[rows], w[0, :, s])
            act_grad = nn(cb[rows], w[1, :, s])
            finish(slot, s, pre, act_grad)

    def finish(slot, s, pre, act_grad):
        rows = slice(slot * TB, (slot + 1) * TB)
        rect = jnp.maximum(pre, 0.0)
        grad = 2.0 * rect * act_grad
        pg[rows, s] = grad.astype(BF16)
        tr[0, s, rows] = grad.T.astype(BF16)
        tr[1, s, rows] = (rect * rect).T.astype(BF16)

    def partial(lo, hi):
        rows = slice(lo * TB, hi * TB)

        @pl.loop(0, NZ, unroll=2)
        def _(k):
            lane = cols(k, DZ)
            g[rows, lane] = nt(pg[rows, :], w[0, lane, :]).astype(BF16)

    forward(ME)
    fcx["r"] = pass_x(cb, R, c_x["r"])
    lo, hi = blk(cb, OPP, x, 0, HALF), blk(cb, OPP, x, HALF)
    c2 = send(lo, lo, XR).send(hi, hi, XL)
    c3 = send(hi, hi, XR).send(lo, lo, XL)
    partial(ME, L)
    pass_y(xb, xr, x_y["r"], fxy, *MID)
    fxy2 = pass_y(xb, x2, x_y["2"])
    fcx["l"].wait()
    forward(L)
    fcx["r"].wait()
    forward(R)
    fcx["2"] = pass_x(cb, OPP, c2)
    partial(L, OPP)
    fxym.wait()
    mid = blk(xb, OPP, x, *MID)
    fmid = send(mid, mid, XR).send(mid, mid, XL)

    def part(slot, r, n, lane=slice(None)):
        return g.at[slot * TB + r:slot * TB + r + n, lane]

    h1b = Batch()
    h1b.send(part(R, 64, 64), rb.at[0, 64:128, :], YR)
    h1b.send(part(L, 0, 64), rb.at[1, 0:64, :], YL)
    far, right, left = cols(x2, FX), cols(xr, FX), cols(xl, FX)
    h2, h2b = {}, Batch()

    def first_x(slots):
        batch = Batch()
        for slot in slots:
            batch.send(part(slot, 128, 64, far), re.at[0, slot], XR)
            batch.send(part(slot, 192, 64, far), re.at[1, slot], XL)
            h2[slot] = batch
        return batch

    def next_x(slot):
        h2b.send(part(slot, 192, 64, right), rf.at[0, slot, 64:128], XR)
        h2b.send(part(slot, 128, 64, left), rf.at[1, slot, 0:64], XL)

    def last_x(slot):
        sf[0, slot] = (part(slot, 128, 64, right)[...].astype(F32) + re[0, slot].astype(F32)).astype(BF16)
        h2b.send(sf.at[0, slot], rf.at[0, slot, 0:64], XR)
        sf[1, slot] = (part(slot, 192, 64, left)[...].astype(F32) + re[1, slot].astype(F32)).astype(BF16)
        h2b.send(sf.at[1, slot], rf.at[1, slot, 64:128], XL)

    h2early = first_x((ME, L, R))
    for slot in (ME, L, R):
        next_x(slot)

    down = ([(0, 4), (1, 3), (0, 3), (1, 2), (0, 2), (1, 1), (0, 1)],
            [(1, 4), (0, 3), (1, 3), (0, 2), (1, 2), (0, 1), (1, 1)])
    todo = []
    for i in range(7):
        for way in range(2):
            u, k = down[way][i]
            todo.append((u, k if way == 0 else -k))
    todo += [(0, 0), (1, 0)]
    wsum = []

    def term(n, rows, lo, hi):
        u, k = todo[n]
        return nn(tr[u, rows, lo * TB:hi * TB], (xb, cb)[u][lo * TB:hi * TB, cols(step(z, k, NZ), DZ)])

    def early(*which):
        for n in which:
            gp[n] = term(n, slice(None), 0, 3)

    def give(batch, n, value):
        u, k = todo[n]
        az = step(z, k, NZ)
        gs[u, az] = value.astype(BF16)
        batch.send(gs.at[u, az], pb.at[u, az], PC)

    def keep(n, value):
        u, k = todo[n]
        gt[u, step(z, k, NZ)] = value

    def give_pair(i):
        batch = Batch()
        for n in (2 * i, 2 * i + 1):
            give(batch, n, gp[n, HB:] + term(n, slice(HB, 2 * HB), 3, 4))
        wsum.append(batch)

    def keep_pair(i):
        for n in (2 * i, 2 * i + 1):
            keep(n, gp[n, :HB] + term(n, slice(0, HB), 3, 4))

    def chunks(i):
        batch = Batch()
        for n in (2 * i, 2 * i + 1):
            value = gp[n] + term(n, slice(None), 3, 4)
            give(batch, n, value[HB:])
            keep(n, value[:HB])
        wsum.append(batch)

    early(*range(14))

    orow = slice(OPP * TB, OPP * TB + TB)
    c3.wait()
    fcx["2"].wait()
    for h in range(2):
        s = slice(h * HB, (h + 1) * HB)
        acc[1, :, s] = nn(cb[orow], w[1, :, s])
    early(14, 15)
    fxy.wait()
    fmid.wait()
    for n, ax in enumerate((x, xl, xr)):
        lane = cols(ax, FX)
        more = nn(xb[orow, lane], w[0, lane, :])
        acc[0] = more if n == 0 else acc[0] + more
    fxy2.wait()
    for h in (1, 0):
        s = slice(h * HB, (h + 1) * HB)
        finish(OPP, s, acc[0, :, s] + nn(xb[orow, far], w[0, far, s]), acc[1, :, s])
        if h == 1:
            give_pair(0)
            give_pair(1)

    gz = []

    away = 1 - lax.div(y, 2)
    sides = (cols(away, DZ // 2), cols(1 - away, DZ // 2))

    def total(u, k, lane):
        az = step(z, k, NZ)
        return gt[u, az, :, lane] + pb[u, az, :, lane].astype(F32)

    def gsend(i):
        wsum[i].wait()
        halves = []
        for half, lane in enumerate(sides):
            if i >= 2:
                gz[i - 2][half].wait()
            batch = Batch()
            for way in range(2):
                u, k = down[way][i]
                value = total(u, k if way == 0 else -k, lane)
                if i >= 2:
                    value = value + rz[way, i - 2, :, lane].astype(F32)
                sz[way, i, :, lane] = value.astype(BF16)
                ref = (way, i, slice(None), lane)
                batch.send(sz.at[ref], rz.at[ref], (ZR, ZL)[way])
            halves.append(batch)
        gz.append(halves)

    keep_pair(0)
    keep_pair(1)
    gsend(0)
    partial(OPP, OPP + 1)
    h1 = []
    for r in (0, 32):
        h1.append(send(part(OPP, r, 32), ra.at[0, r:r + 32], YR)
                  .send(part(OPP, 64 + r, 32), ra.at[1, r:r + 32], YL))
    first_x((OPP,))
    next_x(OPP)
    gsend(1)
    h2early.wait()
    for slot in (ME, L, R):
        last_x(slot)
    chunks(2)
    gsend(2)
    chunks(3)
    def next_y(n, r):
        h1[n].wait()
        sb[0, r:r + 32] = (part(R, r, 32)[...].astype(F32) + ra[0, r:r + 32].astype(F32)).astype(BF16)
        h1b.send(sb.at[0, r:r + 32], rb.at[0, r:r + 32, :], YR)
        sb[1, r:r + 32] = (part(L, 64 + r, 32)[...].astype(F32) + ra[1, r:r + 32].astype(F32)).astype(BF16)
        h1b.send(sb.at[1, r:r + 32], rb.at[1, 64 + r:96 + r, :], YL)

    next_y(0, 0)
    gsend(3)
    h2[OPP].wait()
    last_x(OPP)
    next_y(1, 32)
    chunks(4)
    gsend(4)
    chunks(5)
    gsend(5)

    h2b.wait()
    here = cols(x, FX)
    for slot in range(4):
        q2[slot] = (part(slot, 128, 128, here)[...].astype(F32)
                    + rf[0, slot].astype(F32) + rf[1, slot].astype(F32))
    sh[0] = q2[OPP].astype(BF16)
    sh[1, 64:128] = q2[R, 64:128, :].astype(BF16)
    sh[2, 0:64] = q2[L, 0:64, :].astype(BF16)
    v2 = send(sh.at[0, 0:64, :], rg.at[0], YR).send(sh.at[0, 64:128, :], rg.at[1], YL)
    v2b = Batch()
    v2b.send(sh.at[1, 64:128, :], rh.at[0, 64:128, :], YR)
    v2b.send(sh.at[2, 0:64, :], rh.at[1, 0:64, :], YL)
    chunks(6)
    chunks(7)
    h1b.wait()
    for k in range(NX):
        s = slice(k * FX, (k + 1) * FX)
        q1[k] = g[0:128, s].astype(F32) + rb[0, :, s].astype(F32) + rb[1, :, s].astype(F32)
    sd[0] = q1[x2].astype(BF16)
    sd[1, 64:128] = q1[xr, 64:128, :].astype(BF16)
    sd[2, 0:64] = q1[xl, 0:64, :].astype(BF16)
    v1 = send(sd.at[0, 0:64, :], rc.at[0], XR).send(sd.at[0, 64:128, :], rc.at[1], XL)
    v1b = Batch()
    v1b.send(sd.at[1, 64:128, :], rd.at[0, 64:128, :], XR)
    v1b.send(sd.at[2, 0:64, :], rd.at[1, 0:64, :], XL)
    gsend(6)
    v2.wait()
    sh[1, 0:64] = (q2[R, 0:64, :] + rg[0].astype(F32)).astype(BF16)
    v2b.send(sh.at[1, 0:64, :], rh.at[0, 0:64, :], YR)
    sh[2, 64:128] = (q2[L, 64:128, :] + rg[1].astype(F32)).astype(BF16)
    v2b.send(sh.at[2, 64:128, :], rh.at[1, 64:128, :], YL)
    v1.wait()
    sd[1, 0:64] = (q1[xr, 0:64, :] + rc[0].astype(F32)).astype(BF16)
    v1b.send(sd.at[1, 0:64, :], rd.at[0, 0:64, :], XR)
    sd[2, 64:128] = (q1[xl, 64:128, :] + rc[1].astype(F32)).astype(BF16)
    v1b.send(sd.at[2, 64:128, :], rd.at[1, 64:128, :], XL)
    own, other = cols(c, 256), cols(o, 256)
    ends = Batch()
    def finish_rows(r, value, n):
        q1[n] = value
        fp[r:r + 128] = q1[n, :, other].astype(BF16)
        row = pl.ds(pl.multiple_of(c * TB + r, 128), 128)
        ends.send(fp.at[r:r + 128], og.at[row, :], PC)
        og[row, :] = q1[n, :, own].astype(BF16)

    scale = 1.0 / 128.0
    ops = Batch()
    wsum[7].wait()
    there = cols(y, HB)
    for half, lane in enumerate(sides):
        gz[5][half].wait()
        gz[6][half].wait()
        for u in range(2):
            value = total(u, 0, lane)
            value = value + rz[0, 6 - u, :, lane].astype(F32) + rz[1, 5 + u, :, lane].astype(F32)
            fs_s[u, half] = (value * scale).T.astype(BF16)
            if half == 0:
                odd = lax.rem(y, 2)
                near = 1 - odd
                ops.send(fs_s.at[u, 0, cols(odd, RY), :], ow.at[u, :, there], Y2, small=True)
                ops.send(fs_s.at[u, 0, cols(near, RY), :], ow.at[u, :, there], ACROSS, small=True)
            else:
                odd = lax.rem(y, 2)
                ops.send(fs_s.at[u, 1, cols(1 - odd, RY), :], ow.at[u, :, there], MATE, small=True)
                ow[u, :, there] = fs_s[u, 1, cols(odd, RY), :]

    v1b.wait()
    finish_rows(0, q1[x] + rd[0].astype(F32) + rd[1].astype(F32), 0)
    v2b.wait()
    finish_rows(128, q2[ME] + rh[0].astype(F32) + rh[1].astype(F32), 1)

    ops.wait()
    ends.wait()
    for k, (n, _) in enumerate(groups):
        ref = span(n)
        pltpu.make_async_copy(ref, ref, ssem.at[k]).wait()


def finisher(ow, og, ig_out, ug_out, dg_out, fv, sem):
    stores = [pltpu.make_async_copy(og, ig_out, sem.at[0])]
    stores[0].start()
    for u, out in ((0, ug_out), (1, dg_out)):
        fv[u] = ow[u].astype(F32)
        stores.append(pltpu.make_async_copy(fv.at[u], out, sem.at[1 + u]))
        stores[-1].start()
    for copy in stores:
        copy.wait()


def per_device(normed_input, cotangent, up_weight, down_weight):
    bf = lambda *s: pltpu.VMEM(s, BF16)
    f4 = lambda *s: pltpu.VMEM(s, F32)
    hbm = pl.BlockSpec(memory_space=pl.ANY)
    vmem = pl.BlockSpec(memory_space=pltpu.VMEM)
    shape = jax.ShapeDtypeStruct
    ow, og = pl.pallas_call(
        kernel,
        out_shape=(bf(2, RY, 4 * HB), bf(2 * TB, 256)),
        in_specs=[hbm] * 4,
        out_specs=(vmem,) * 2,
        scratch_shapes=[
            bf(NY * TB, D), bf(NY * TB, D),
            bf(2, D, 2 * HB),
            bf(TB, 256), bf(TB, 256),
            bf(2, RY, 4 * HB),
            bf(NY * TB, 2 * HB),
            bf(2, 2 * HB, NY * TB),
            f4(2, TB, 2 * HB),
            f4(2 * NZ, 2 * HB, DZ),
            f4(2, NZ, HB, DZ),
            bf(2, NZ, HB, DZ), bf(2, NZ, HB, DZ),
            bf(2, 7, HB, DZ), bf(2, 7, HB, DZ),
            bf(2, 2, DZ // 2, HB),
            bf(NY * TB, D),
            bf(2, 64, D), bf(2, 128, D), bf(2, 64, D),
            f4(NX, 128, FX),
            bf(2, 64, FX), bf(2, 128, FX), bf(3, 128, FX),
            bf(2, NY, 64, FX), bf(2, NY, 128, FX), bf(2, NY, 64, FX),
            f4(NY, 128, FX),
            bf(2, 64, FX), bf(2, 128, FX), bf(3, 128, FX),
            bf(TB, 256),
            pltpu.SemaphoreType.DMA((5,)),
            pltpu.SemaphoreType.DMA((SENDS,)),
            pltpu.SemaphoreType.DMA((RECVS,)),
        ],
        compiler_params=pltpu.CompilerParams(
            collective_id=0, has_side_effects=True, vmem_limit_bytes=60 * 1024 * 1024
        ),
    )(normed_input, cotangent, up_weight, down_weight.T)
    ig, ug, dg = pl.pallas_call(
        finisher,
        out_shape=(shape((2 * TB, 256), BF16), shape((RY, 4 * HB), F32), shape((RY, 4 * HB), F32)),
        in_specs=[vmem] * 2,
        out_specs=(hbm,) * 3,
        scratch_shapes=[f4(2, RY, 4 * HB), pltpu.SemaphoreType.DMA((3,))],
    )(*(pltpu.with_memory_space_constraint(a, pltpu.VMEM) for a in (ow, og)))
    return ig, ug, dg.T


def solution(mesh):
    return jax.shard_map(
        per_device, mesh=mesh,
        in_specs=(P("fs", "tp"), P("fs", "tp"), P("fs", "tp"), P("tp", "fs")),
        out_specs=(P("fs", "tp"), P("fs", "tp"), P("tp", "fs")),
        check_vma=False,
    )
```

```python
import math

import jax
import jax.numpy as jnp
from jax import lax
from jax.experimental import pallas as pl
from jax.experimental.pallas import tpu as pltpu
from jax.sharding import PartitionSpec as P

NX, NY, NZ = 4, 4, 8
D = 2048
TB = 256
FX = 512
HB = 256
DZ = 256
RY = 64
HALF = TB // 2
CUT = 112
MID = (96, 160)
SENDS, RECVS = 6, 67
MESH = pl.DeviceIdType.MESH
BF16, F32 = jnp.bfloat16, jnp.float32


def nn(a, b):
    return lax.dot_general(a, b, (((1,), (0,)), ((), ())), preferred_element_type=F32)


def nt(a, b):
    return lax.dot_general(a, b, (((1,), (1,)), ((), ())), preferred_element_type=F32)


def kernel(
    x_in, c_in, up_in, dn_in, ow, og,
    xb, cb, w, xs, cs, uv, pg, tr, acc, gp, gt, gs, pb, rz, sz, fs_s, g,
    ra, rb, sb, q1, rc, rd, sd, re, rf, sf, q2, rg, rh, sh, fp,
    lsem, ssem, rsem,
):
    fs, tp = lax.axis_index("fs"), lax.axis_index("tp")
    z, y = lax.div(fs, NY), lax.rem(fs, NY)
    x, c = lax.div(tp, 2), lax.rem(tp, 2)
    o = 1 - c
    step = lambda a, k, n: lax.rem(a + (k % n), n)
    xr, xl, x2 = step(x, 1, NX), step(x, -1, NX), step(x, 2, NX)
    yr, yl, y2 = step(y, 1, NY), step(y, -1, NY), step(y, 2, NY)
    at = lambda ax, ay, az, ac: (az * NY + ay, ax * 2 + ac)
    XR, XL = at(xr, y, z, c), at(xl, y, z, c)
    YR, YL, Y2 = at(x, yr, z, c), at(x, yl, z, c), at(x, y2, z, c)
    ZR, ZL = at(x, y, step(z, 1, NZ), c), at(x, y, step(z, -1, NZ), c)
    PC = at(x, y, z, o)
    mate = y + 1 - 2 * lax.rem(y, 2)
    MATE, ACROSS = at(x, mate, z, c), at(x, step(mate, 2, NY), z, c)
    ME, L, R, OPP = range(4)

    arrivals = iter(range(RECVS))
    groups = []
    SPAN = 4 << 20

    def size(ref):
        return math.prod(ref.shape) * 2

    def span(count):
        return xb.at[0:count // (2 * D), :]

    class Batch:
        def __init__(self):
            self.sem, self.bytes = rsem.at[next(arrivals)], 0

        def send(self, src, dst, where, small=False):
            n = size(src)
            at = next((k for k, g in enumerate(groups) if g[1] == small and g[0] + n <= SPAN), None)
            if at is None:
                at = len(groups)
                groups.append([0, small])
            groups[at][0] += n
            self.bytes += n
            pltpu.make_async_remote_copy(
                src_ref=src, dst_ref=dst, send_sem=ssem.at[at], recv_sem=self.sem,
                device_id=where, device_id_type=MESH,
            ).start()
            return self

        def wait(self):
            ref = span(self.bytes)
            pltpu.make_async_copy(ref, ref, self.sem).wait()

    def send(src, dst, where):
        return Batch().send(src, dst, where)

    def cols(k, n):
        return pl.ds(pl.multiple_of(k * n, n), n)

    mine = pl.ds(pl.multiple_of(x * FX + c * 256, 256), 256)
    wrow = pl.ds(pl.multiple_of(z * DZ + y * RY, RY), RY)
    loads = []
    for i, pairs in enumerate((
        ((c_in.at[cols(o, TB), :], cs),),
        ((x_in.at[cols(o, TB), :], xs),),
        ((up_in, uv.at[0]), (dn_in, uv.at[1])),
        ((c_in.at[cols(c, TB), :], cb.at[0:TB, mine]), (x_in.at[cols(c, TB), :], xb.at[0:TB, mine])),
        ((up_in.at[:, cols(y, HB)], w.at[0, wrow, 0:HB]),
         (dn_in.at[:, cols(y, HB)], w.at[1, wrow, 0:HB])),
    )):
        for src, dst in pairs:
            pltpu.make_async_copy(src, dst, lsem.at[i]).start()
        ref = span(sum(size(dst) for _, dst in pairs))
        loads.append(pltpu.make_async_copy(ref, ref, lsem.at[i]))

    barrier = pltpu.get_barrier_semaphore()
    peers = (XR, XL, YR, YL, Y2, ZR, ZL, PC)
    for peer in peers:
        pl.semaphore_signal(barrier, inc=1, device_id=peer, device_id_type=MESH)
    pl.semaphore_wait(barrier, len(peers))

    loads[0].wait()
    cop = send(cs, cb.at[0:TB, mine], PC)
    loads[1].wait()
    xop = send(xs, xb.at[0:TB, mine], PC)
    loads[2].wait()
    loads[3].wait()
    x_x = Batch()
    for way in (XR, XL):
        x_x.send(xb.at[0:TB, mine], xb.at[0:TB, mine], way)
    wops = Batch()
    for ay, where in ((y2, Y2), (yr, YR), (yl, YL)):
        for u in range(2):
            wops.send(uv.at[u, :, cols(ay, HB)], w.at[u, wrow, 0:HB], where, small=True)

    def blk(buf, slot, ax, lo=0, hi=TB):
        return buf.at[slot * TB + lo:slot * TB + hi, cols(ax, FX)]

    def over_x(buf, slot, ax):
        ref = blk(buf, slot, ax)
        return send(ref, ref, XR).send(ref, ref, XL)

    def over_y(buf, ax):
        ref = blk(buf, ME, ax)
        return send(ref, blk(buf, L, ax), YR).send(ref, blk(buf, R, ax), YL)

    def pass_x(buf, slot, batch):
        batch.wait()
        a, b = blk(buf, slot, xl, 0, HALF), blk(buf, slot, xr, HALF)
        return send(a, a, XR).send(b, b, XL)

    def pass_y(buf, ax, batch, out=None, lo=CUT, hi=CUT):
        batch.wait()
        out = out or Batch()
        out.send(blk(buf, L, ax, 0, lo), blk(buf, OPP, ax, 0, lo), YR)
        return out.send(blk(buf, R, ax, hi), blk(buf, OPP, ax, hi), YL)

    cop.wait()
    c_y = over_y(cb, x)
    there = pl.ds(pl.multiple_of(x * FX + o * 256, 256), 256)
    xop.wait()
    for way in (XR, XL):
        x_x.send(xb.at[0:TB, there], xb.at[0:TB, there], way)
    x_y = {"me": over_y(xb, x)}
    c_x = {"me": over_x(cb, ME, x)}

    loads[4].wait()
    wops.wait()

    wz = []
    wpc = Batch()
    order = ([(0, 0), (1, 0), (0, 1), (1, 1), (0, 2), (1, 2), (0, 3)],
             [(1, 0), (0, 0), (1, 1), (0, 1), (1, 2), (0, 2), (1, 3)])

    def wsend(i):
        batch = Batch()
        for way in range(2):
            u, k = order[way][i]
            ref = w.at[u, cols(step(z, -k if way == 0 else k, NZ), DZ), 0:HB]
            batch.send(ref, ref, (ZR, ZL)[way])
        wz.append(batch)

    def wpair(u, k):
        rows = cols(step(z, k, NZ), DZ)
        wpc.send(w.at[u, rows, 0:HB], w.at[u, rows, HB:2 * HB], PC)

    wsend(0)
    wsend(1)
    for u in range(2):
        wpair(u, 0)

    def warrive(i):
        wz[i].wait()
        if i + 2 < 7:
            wsend(i + 2)
        for way in range(2):
            u, k = order[way][i]
            wpair(u, -(k + 1) if way == 0 else k + 1)

    fx = pass_x(xb, ME, x_x)
    warrive(0)
    fc = pass_y(cb, x, c_y)
    x_y["l"] = over_y(xb, xl)
    x_y["r"] = over_y(xb, xr)
    warrive(1)
    fcx = {"me": pass_x(cb, ME, c_x["me"])}
    c_x["l"] = over_x(cb, L, x)
    c_x["r"] = over_x(cb, R, x)
    warrive(2)
    fx.wait()
    x_y["2"] = over_y(xb, x2)
    warrive(3)
    fxym = pass_y(xb, x, x_y["me"])
    fc.wait()
    warrive(4)
    warrive(5)
    fcx["l"] = pass_x(cb, L, c_x["l"])
    fxy = pass_y(xb, xl, x_y["l"], None, *MID)
    warrive(6)
    fcx["me"].wait()
    wpc.wait()

    def forward(slot):
        rows = slice(slot * TB, (slot + 1) * TB)
        for h in range(2):
            s = slice(h * HB, (h + 1) * HB)
            pre = nn(xb[rows], w[0, :, s])
            act_grad = nn(cb[rows], w[1, :, s])
            finish(slot, s, pre, act_grad)

    def finish(slot, s, pre, act_grad):
        rows = slice(slot * TB, (slot + 1) * TB)
        rect = jnp.maximum(pre, 0.0)
        grad = 2.0 * rect * act_grad
        pg[rows, s] = grad.astype(BF16)
        tr[0, s, rows] = grad.T.astype(BF16)
        tr[1, s, rows] = (rect * rect).T.astype(BF16)

    def partial(lo, hi):
        rows = slice(lo, hi)

        @pl.loop(0, NZ, unroll=4)
        def _(k):
            lane = cols(k, DZ)
            g[rows, lane] = nt(pg[rows, :], w[0, lane, :]).astype(BF16)

    forward(ME)
    fcx["r"] = pass_x(cb, R, c_x["r"])
    lo, hi = blk(cb, OPP, x, 0, HALF), blk(cb, OPP, x, HALF)
    c2 = send(lo, lo, XR).send(hi, hi, XL)
    c3 = send(hi, hi, XR).send(lo, lo, XL)
    partial(ME * TB, L * TB)
    pass_y(xb, xr, x_y["r"], fxy, *MID)
    fxy2 = pass_y(xb, x2, x_y["2"])
    fcx["l"].wait()
    forward(L)
    fcx["r"].wait()
    forward(R)
    fcx["2"] = pass_x(cb, OPP, c2)
    partial(L * TB, OPP * TB)
    fxym.wait()
    mid = blk(xb, OPP, x, *MID)
    fmid = send(mid, mid, XR).send(mid, mid, XL)

    def part(slot, r, n, lane=slice(None)):
        return g.at[slot * TB + r:slot * TB + r + n, lane]

    h1b = Batch()
    h1b.send(part(R, 64, 64), rb.at[0, 64:128, :], YR)
    h1b.send(part(L, 0, 64), rb.at[1, 0:64, :], YL)
    far, right, left = cols(x2, FX), cols(xr, FX), cols(xl, FX)
    h2, h2b = {}, Batch()

    def first_x(slots):
        batch = Batch()
        for slot in slots:
            batch.send(part(slot, 128, 64, far), re.at[0, slot], XR)
            batch.send(part(slot, 192, 64, far), re.at[1, slot], XL)
            h2[slot] = batch
        return batch

    def next_x(slot):
        h2b.send(part(slot, 192, 64, right), rf.at[0, slot, 64:128], XR)
        h2b.send(part(slot, 128, 64, left), rf.at[1, slot, 0:64], XL)

    def last_x(slot):
        sf[0, slot] = (part(slot, 128, 64, right)[...].astype(F32) + re[0, slot].astype(F32)).astype(BF16)
        h2b.send(sf.at[0, slot], rf.at[0, slot, 0:64], XR)
        sf[1, slot] = (part(slot, 192, 64, left)[...].astype(F32) + re[1, slot].astype(F32)).astype(BF16)
        h2b.send(sf.at[1, slot], rf.at[1, slot, 64:128], XL)

    h2early = first_x((ME, L, R))
    for slot in (ME, L, R):
        next_x(slot)

    down = ([(0, 4), (1, 3), (0, 3), (1, 2), (0, 2), (1, 1), (0, 1)],
            [(1, 4), (0, 3), (1, 3), (0, 2), (1, 2), (0, 1), (1, 1)])
    todo = []
    for i in range(7):
        for way in range(2):
            u, k = down[way][i]
            todo.append((u, k if way == 0 else -k))
    todo += [(0, 0), (1, 0)]
    wsum = []

    def term(n, rows, lo, hi):
        u, k = todo[n]
        return nn(tr[u, rows, lo * TB:hi * TB], (xb, cb)[u][lo * TB:hi * TB, cols(step(z, k, NZ), DZ)])

    def early(*which):
        for n in which:
            gp[n] = term(n, slice(None), 0, 3)

    def give(batch, n, value):
        u, k = todo[n]
        az = step(z, k, NZ)
        gs[u, az] = value.astype(BF16)
        batch.send(gs.at[u, az], pb.at[u, az], PC)

    def keep(n, value):
        u, k = todo[n]
        gt[u, step(z, k, NZ)] = value

    def give_pair(i):
        batch = Batch()
        for n in (2 * i, 2 * i + 1):
            give(batch, n, gp[n, HB:] + term(n, slice(HB, 2 * HB), 3, 4))
        wsum.append(batch)

    def keep_pair(i):
        for n in (2 * i, 2 * i + 1):
            keep(n, gp[n, :HB] + term(n, slice(0, HB), 3, 4))

    def chunks(i):
        batch = Batch()
        for n in (2 * i, 2 * i + 1):
            value = gp[n] + term(n, slice(None), 3, 4)
            give(batch, n, value[HB:])
            keep(n, value[:HB])
        wsum.append(batch)

    early(*range(14))

    orow = slice(OPP * TB, OPP * TB + TB)
    c3.wait()
    fcx["2"].wait()
    for h in range(2):
        s = slice(h * HB, (h + 1) * HB)
        acc[1, :, s] = nn(cb[orow], w[1, :, s])
    early(14, 15)
    fxy.wait()
    fmid.wait()
    for n, ax in enumerate((x, xl, xr)):
        lane = cols(ax, FX)
        more = nn(xb[orow, lane], w[0, lane, :])
        acc[0] = more if n == 0 else acc[0] + more
    fxy2.wait()
    for h in (1, 0):
        s = slice(h * HB, (h + 1) * HB)
        finish(OPP, s, acc[0, :, s] + nn(xb[orow, far], w[0, far, s]), acc[1, :, s])
        if h == 1:
            give_pair(0)

    gz = []

    away = 1 - lax.div(y, 2)
    sides = (cols(away, DZ // 2), cols(1 - away, DZ // 2))

    WHOLE, TOP, LOW = slice(None), slice(0, HB // 2), slice(HB // 2, HB)

    def total(u, k, lane, rows=WHOLE):
        az = step(z, k, NZ)
        return gt[u, az, rows, lane] + pb[u, az, rows, lane].astype(F32)

    def gsend(i, halves=(0, 1)):
        if 0 in halves:
            wsum[i].wait()
            gz.append([])
        for half in halves:
            lane = sides[half]
            if i >= 2:
                gz[i - 2][half].wait()
            for rows in (TOP, LOW) if (i, half) == (6, 1) else (WHOLE,):
                batch = Batch()
                for way in range(2):
                    u, k = down[way][i]
                    value = total(u, k if way == 0 else -k, lane, rows)
                    if i >= 2:
                        value = value + rz[way, i - 2, rows, lane].astype(F32)
                    sz[way, i, rows, lane] = value.astype(BF16)
                    ref = (way, i, rows, lane)
                    batch.send(sz.at[ref], rz.at[ref], (ZR, ZL)[way])
                gz[i].append(batch)

    keep_pair(0)
    partial(OPP * TB, OPP * TB + HALF)
    h1 = []
    for r in (0, 32):
        h1.append(send(part(OPP, r, 32), ra.at[0, r:r + 32], YR)
                  .send(part(OPP, 64 + r, 32), ra.at[1, r:r + 32], YL))
    gsend(0)
    chunks(1)
    partial(OPP * TB + HALF, OPP * TB + TB)
    first_x((OPP,))
    next_x(OPP)
    gsend(1)
    h2early.wait()
    for slot in (ME, L, R):
        last_x(slot)
    chunks(2)
    gsend(2)
    chunks(3)
    def next_y(n, r):
        h1[n].wait()
        sb[0, r:r + 32] = (part(R, r, 32)[...].astype(F32) + ra[0, r:r + 32].astype(F32)).astype(BF16)
        h1b.send(sb.at[0, r:r + 32], rb.at[0, r:r + 32, :], YR)
        sb[1, r:r + 32] = (part(L, 64 + r, 32)[...].astype(F32) + ra[1, r:r + 32].astype(F32)).astype(BF16)
        h1b.send(sb.at[1, r:r + 32], rb.at[1, 64 + r:96 + r, :], YL)

    next_y(0, 0)
    gsend(3)
    h2[OPP].wait()
    last_x(OPP)
    next_y(1, 32)
    chunks(4)
    gsend(4)
    chunks(5)
    chunks(6)
    gsend(5, (0,))

    h2b.wait()
    here = cols(x, FX)
    for slot in range(4):
        q2[slot] = (part(slot, 128, 128, here)[...].astype(F32)
                    + rf[0, slot].astype(F32) + rf[1, slot].astype(F32))
    sh[0] = q2[OPP].astype(BF16)
    sh[1, 64:128] = q2[R, 64:128, :].astype(BF16)
    sh[2, 0:64] = q2[L, 0:64, :].astype(BF16)
    v2 = send(sh.at[0, 0:64, :], rg.at[0], YR).send(sh.at[0, 64:128, :], rg.at[1], YL)
    v2b = Batch()
    v2b.send(sh.at[1, 64:128, :], rh.at[0, 64:128, :], YR)
    v2b.send(sh.at[2, 0:64, :], rh.at[1, 0:64, :], YL)
    chunks(7)
    h1b.wait()
    for k in range(NX):
        s = slice(k * FX, (k + 1) * FX)
        q1[k] = g[0:128, s].astype(F32) + rb[0, :, s].astype(F32) + rb[1, :, s].astype(F32)
    sd[0] = q1[x2].astype(BF16)
    sd[1, 64:128] = q1[xr, 64:128, :].astype(BF16)
    sd[2, 0:64] = q1[xl, 0:64, :].astype(BF16)
    v1 = send(sd.at[0, 0:64, :], rc.at[0], XR).send(sd.at[0, 64:128, :], rc.at[1], XL)
    v1b = Batch()
    v1b.send(sd.at[1, 64:128, :], rd.at[0, 64:128, :], XR)
    v1b.send(sd.at[2, 0:64, :], rd.at[1, 0:64, :], XL)
    gsend(6, (0,))
    gsend(5, (1,))
    gsend(6, (1,))
    v2.wait()
    sh[1, 0:64] = (q2[R, 0:64, :] + rg[0].astype(F32)).astype(BF16)
    v2b.send(sh.at[1, 0:64, :], rh.at[0, 0:64, :], YR)
    sh[2, 64:128] = (q2[L, 64:128, :] + rg[1].astype(F32)).astype(BF16)
    v2b.send(sh.at[2, 64:128, :], rh.at[1, 64:128, :], YL)
    v1.wait()
    sd[1, 0:64] = (q1[xr, 0:64, :] + rc[0].astype(F32)).astype(BF16)
    v1b.send(sd.at[1, 0:64, :], rd.at[0, 0:64, :], XR)
    sd[2, 64:128] = (q1[xl, 64:128, :] + rc[1].astype(F32)).astype(BF16)
    v1b.send(sd.at[2, 64:128, :], rd.at[1, 64:128, :], XL)
    own, other = cols(c, 256), cols(o, 256)
    ends = Batch()
    def finish_rows(r, value, n):
        q1[n] = value
        fp[r:r + 128] = q1[n, :, other].astype(BF16)
        row = pl.ds(pl.multiple_of(c * TB + r, 128), 128)
        ends.send(fp.at[r:r + 128], og.at[row, :], PC)
        og[row, :] = q1[n, :, own].astype(BF16)

    scale = 1.0 / 128.0
    ops = Batch()
    wsum[7].wait()
    there = cols(y, HB)
    odd = lax.rem(y, 2)
    near = 1 - odd

    def zlast(u, lane, rows=WHOLE):
        value = total(u, 0, lane, rows)
        value = value + rz[0, 6 - u, rows, lane].astype(F32) + rz[1, 5 + u, rows, lane].astype(F32)
        return (value * scale).T.astype(BF16)

    gz[5][0].wait()
    gz[6][0].wait()
    for u in range(2):
        fs_s[u, 0] = zlast(u, sides[0])
        ops.send(fs_s.at[u, 0, cols(odd, RY), :], ow.at[u, :, there], Y2, small=True)
        ops.send(fs_s.at[u, 0, cols(near, RY), :], ow.at[u, :, there], ACROSS, small=True)
    gz[5][1].wait()
    for part_of, rows in enumerate((TOP, LOW)):
        gz[6][1 + part_of].wait()
        lane = pl.ds(pl.multiple_of(y * HB + part_of * 128, 128), 128)
        for u in range(2):
            fs_s[u, 1, :, rows] = zlast(u, sides[1], rows)
            ops.send(fs_s.at[u, 1, cols(near, RY), rows], ow.at[u, :, lane], MATE, small=True)
    for u in range(2):
        ow[u, :, there] = fs_s[u, 1, cols(odd, RY), :]

    v1b.wait()
    finish_rows(0, q1[x] + rd[0].astype(F32) + rd[1].astype(F32), 0)
    v2b.wait()
    finish_rows(128, q2[ME] + rh[0].astype(F32) + rh[1].astype(F32), 1)

    ops.wait()
    ends.wait()
    for k, (n, _) in enumerate(groups):
        ref = span(n)
        pltpu.make_async_copy(ref, ref, ssem.at[k]).wait()


def finisher(ow, og, ig_out, ug_out, dg_out, fv, sem):
    stores = [pltpu.make_async_copy(og, ig_out, sem.at[0])]
    stores[0].start()
    for u, out in ((0, ug_out), (1, dg_out)):
        fv[u] = ow[u].astype(F32)
        stores.append(pltpu.make_async_copy(fv.at[u], out, sem.at[1 + u]))
        stores[-1].start()
    for copy in stores:
        copy.wait()


def per_device(normed_input, cotangent, up_weight, down_weight):
    bf = lambda *s: pltpu.VMEM(s, BF16)
    f4 = lambda *s: pltpu.VMEM(s, F32)
    hbm = pl.BlockSpec(memory_space=pl.ANY)
    vmem = pl.BlockSpec(memory_space=pltpu.VMEM)
    shape = jax.ShapeDtypeStruct
    ow, og = pl.pallas_call(
        kernel,
        out_shape=(bf(2, RY, 4 * HB), bf(2 * TB, 256)),
        in_specs=[hbm] * 4,
        out_specs=(vmem,) * 2,
        scratch_shapes=[
            bf(NY * TB, D), bf(NY * TB, D),
            bf(2, D, 2 * HB),
            bf(TB, 256), bf(TB, 256),
            bf(2, RY, 4 * HB),
            bf(NY * TB, 2 * HB),
            bf(2, 2 * HB, NY * TB),
            f4(2, TB, 2 * HB),
            f4(2 * NZ, 2 * HB, DZ),
            f4(2, NZ, HB, DZ),
            bf(2, NZ, HB, DZ), bf(2, NZ, HB, DZ),
            bf(2, 7, HB, DZ), bf(2, 7, HB, DZ),
            bf(2, 2, DZ // 2, HB),
            bf(NY * TB, D),
            bf(2, 64, D), bf(2, 128, D), bf(2, 64, D),
            f4(NX, 128, FX),
            bf(2, 64, FX), bf(2, 128, FX), bf(3, 128, FX),
            bf(2, NY, 64, FX), bf(2, NY, 128, FX), bf(2, NY, 64, FX),
            f4(NY, 128, FX),
            bf(2, 64, FX), bf(2, 128, FX), bf(3, 128, FX),
            bf(TB, 256),
            pltpu.SemaphoreType.DMA((5,)),
            pltpu.SemaphoreType.DMA((SENDS,)),
            pltpu.SemaphoreType.DMA((RECVS,)),
        ],
        compiler_params=pltpu.CompilerParams(
            collective_id=0, has_side_effects=True, vmem_limit_bytes=60 * 1024 * 1024
        ),
    )(normed_input, cotangent, up_weight, down_weight.T)
    ig, ug, dg = pl.pallas_call(
        finisher,
        out_shape=(shape((2 * TB, 256), BF16), shape((RY, 4 * HB), F32), shape((RY, 4 * HB), F32)),
        in_specs=[vmem] * 2,
        out_specs=(hbm,) * 3,
        scratch_shapes=[f4(2, RY, 4 * HB), pltpu.SemaphoreType.DMA((3,))],
    )(*(pltpu.with_memory_space_constraint(a, pltpu.VMEM) for a in (ow, og)))
    return ig, ug, dg.T


def solution(mesh):
    return jax.shard_map(
        per_device, mesh=mesh,
        in_specs=(P("fs", "tp"), P("fs", "tp"), P("fs", "tp"), P("tp", "fs")),
        out_specs=(P("fs", "tp"), P("fs", "tp"), P("tp", "fs")),
        check_vma=False,
    )
```

```python
import math

import jax
import jax.numpy as jnp
from jax import lax
from jax.experimental import pallas as pl
from jax.experimental.pallas import tpu as pltpu
from jax.sharding import PartitionSpec as P

NX, NY, NZ = 4, 4, 8
D = 2048
TB = 256
FX = 512
HB = 256
DZ = 256
RY = 64
HALF = TB // 2
CUT = 128
MID = (96, 160)
SENDS, RECVS = 6, 67
MESH = pl.DeviceIdType.MESH
BF16, F32 = jnp.bfloat16, jnp.float32


def nn(a, b):
    return lax.dot_general(a, b, (((1,), (0,)), ((), ())), preferred_element_type=F32)


def nt(a, b):
    return lax.dot_general(a, b, (((1,), (1,)), ((), ())), preferred_element_type=F32)


def kernel(
    x_in, c_in, up_in, dn_in, ow, og,
    xb, cb, w, xs, cs, uv, pg, tr, acc, gp, gt, gs, pb, rz, sz, fs_s, g,
    ra, rb, sb, q1, rc, rd, sd, re, rf, sf, q2, rg, rh, sh, fp,
    lsem, ssem, rsem,
):
    fs, tp = lax.axis_index("fs"), lax.axis_index("tp")
    z, y = lax.div(fs, NY), lax.rem(fs, NY)
    x, c = lax.div(tp, 2), lax.rem(tp, 2)
    o = 1 - c
    step = lambda a, k, n: lax.rem(a + (k % n), n)
    xr, xl, x2 = step(x, 1, NX), step(x, -1, NX), step(x, 2, NX)
    yr, yl, y2 = step(y, 1, NY), step(y, -1, NY), step(y, 2, NY)
    at = lambda ax, ay, az, ac: (az * NY + ay, ax * 2 + ac)
    XR, XL = at(xr, y, z, c), at(xl, y, z, c)
    YR, YL, Y2 = at(x, yr, z, c), at(x, yl, z, c), at(x, y2, z, c)
    ZR, ZL = at(x, y, step(z, 1, NZ), c), at(x, y, step(z, -1, NZ), c)
    PC = at(x, y, z, o)
    mate = y + 1 - 2 * lax.rem(y, 2)
    MATE, ACROSS = at(x, mate, z, c), at(x, step(mate, 2, NY), z, c)
    ME, L, R, OPP = range(4)

    arrivals = iter(range(RECVS))
    groups = []
    SPAN = 4 << 20

    def size(ref):
        return math.prod(ref.shape) * 2

    def span(count):
        return xb.at[0:count // (2 * D), :]

    class Batch:
        def __init__(self):
            self.sem, self.bytes = rsem.at[next(arrivals)], 0

        def send(self, src, dst, where, small=False):
            n = size(src)
            at = next((k for k, g in enumerate(groups) if g[1] == small and g[0] + n <= SPAN), None)
            if at is None:
                at = len(groups)
                groups.append([0, small])
            groups[at][0] += n
            self.bytes += n
            pltpu.make_async_remote_copy(
                src_ref=src, dst_ref=dst, send_sem=ssem.at[at], recv_sem=self.sem,
                device_id=where, device_id_type=MESH,
            ).start()
            return self

        def wait(self):
            ref = span(self.bytes)
            pltpu.make_async_copy(ref, ref, self.sem).wait()

    def send(src, dst, where):
        return Batch().send(src, dst, where)

    def cols(k, n):
        return pl.ds(pl.multiple_of(k * n, n), n)

    mine = pl.ds(pl.multiple_of(x * FX + c * 256, 256), 256)
    wrow = pl.ds(pl.multiple_of(z * DZ + y * RY, RY), RY)
    loads = []
    for i, pairs in enumerate((
        ((c_in.at[cols(o, TB), :], cs),),
        ((x_in.at[cols(o, TB), :], xs),),
        ((up_in, uv.at[0]), (dn_in, uv.at[1])),
        ((c_in.at[cols(c, TB), :], cb.at[0:TB, mine]), (x_in.at[cols(c, TB), :], xb.at[0:TB, mine])),
        ((up_in.at[:, cols(y, HB)], w.at[0, wrow, 0:HB]),
         (dn_in.at[:, cols(y, HB)], w.at[1, wrow, 0:HB])),
    )):
        for src, dst in pairs:
            pltpu.make_async_copy(src, dst, lsem.at[i]).start()
        ref = span(sum(size(dst) for _, dst in pairs))
        loads.append(pltpu.make_async_copy(ref, ref, lsem.at[i]))

    barrier = pltpu.get_barrier_semaphore()
    peers = (XR, XL, YR, YL, Y2, ZR, ZL, PC)
    for peer in peers:
        pl.semaphore_signal(barrier, inc=1, device_id=peer, device_id_type=MESH)
    pl.semaphore_wait(barrier, len(peers))

    loads[0].wait()
    cop = send(cs, cb.at[0:TB, mine], PC)
    loads[1].wait()
    xop = send(xs, xb.at[0:TB, mine], PC)
    loads[2].wait()
    loads[3].wait()
    x_x = Batch()
    for way in (XR, XL):
        x_x.send(xb.at[0:TB, mine], xb.at[0:TB, mine], way)
    wops = Batch()
    for ay, where in ((y2, Y2), (yr, YR), (yl, YL)):
        for u in range(2):
            wops.send(uv.at[u, :, cols(ay, HB)], w.at[u, wrow, 0:HB], where, small=True)

    def blk(buf, slot, ax, lo=0, hi=TB):
        return buf.at[slot * TB + lo:slot * TB + hi, cols(ax, FX)]

    def over_x(buf, slot, ax):
        ref = blk(buf, slot, ax)
        return send(ref, ref, XR).send(ref, ref, XL)

    def over_y(buf, ax):
        ref = blk(buf, ME, ax)
        return send(ref, blk(buf, L, ax), YR).send(ref, blk(buf, R, ax), YL)

    def pass_x(buf, slot, batch):
        batch.wait()
        a, b = blk(buf, slot, xl, 0, HALF), blk(buf, slot, xr, HALF)
        return send(a, a, XR).send(b, b, XL)

    def pass_y(buf, ax, batch, out=None, lo=CUT, hi=CUT):
        batch.wait()
        out = out or Batch()
        out.send(blk(buf, L, ax, 0, lo), blk(buf, OPP, ax, 0, lo), YR)
        return out.send(blk(buf, R, ax, hi), blk(buf, OPP, ax, hi), YL)

    cop.wait()
    c_y = over_y(cb, x)
    there = pl.ds(pl.multiple_of(x * FX + o * 256, 256), 256)
    xop.wait()
    for way in (XR, XL):
        x_x.send(xb.at[0:TB, there], xb.at[0:TB, there], way)
    x_y = {"me": over_y(xb, x)}
    c_x = {"me": over_x(cb, ME, x)}

    loads[4].wait()
    wops.wait()

    wz = []
    wpc = Batch()
    order = ([(0, 0), (1, 0), (0, 1), (1, 1), (0, 2), (1, 2), (0, 3)],
             [(1, 0), (0, 0), (1, 1), (0, 1), (1, 2), (0, 2), (1, 3)])

    def wsend(i):
        batch = Batch()
        for way in range(2):
            u, k = order[way][i]
            ref = w.at[u, cols(step(z, -k if way == 0 else k, NZ), DZ), 0:HB]
            batch.send(ref, ref, (ZR, ZL)[way])
        wz.append(batch)

    def wpair(u, k):
        rows = cols(step(z, k, NZ), DZ)
        wpc.send(w.at[u, rows, 0:HB], w.at[u, rows, HB:2 * HB], PC)

    wsend(0)
    wsend(1)
    for u in range(2):
        wpair(u, 0)

    def warrive(i):
        wz[i].wait()
        if i + 2 < 7:
            wsend(i + 2)
        for way in range(2):
            u, k = order[way][i]
            wpair(u, -(k + 1) if way == 0 else k + 1)

    fx = pass_x(xb, ME, x_x)
    warrive(0)
    fc = pass_y(cb, x, c_y)
    x_y["l"] = over_y(xb, xl)
    x_y["r"] = over_y(xb, xr)
    warrive(1)
    fcx = {"me": pass_x(cb, ME, c_x["me"])}
    c_x["l"] = over_x(cb, L, x)
    c_x["r"] = over_x(cb, R, x)
    warrive(2)
    fx.wait()
    x_y["2"] = over_y(xb, x2)
    warrive(3)
    fxym = pass_y(xb, x, x_y["me"])
    fc.wait()
    warrive(4)
    warrive(5)
    fcx["l"] = pass_x(cb, L, c_x["l"])
    fxy = pass_y(xb, xl, x_y["l"], None, *MID)
    warrive(6)
    fcx["me"].wait()
    wpc.wait()

    def forward(slot):
        rows = slice(slot * TB, (slot + 1) * TB)
        for h in range(2):
            s = slice(h * HB, (h + 1) * HB)
            pre = nn(xb[rows], w[0, :, s])
            act_grad = nn(cb[rows], w[1, :, s])
            finish(slot, s, pre, act_grad)

    def finish(slot, s, pre, act_grad):
        rows = slice(slot * TB, (slot + 1) * TB)
        rect = jnp.maximum(pre, 0.0)
        grad = 2.0 * rect * act_grad
        pg[rows, s] = grad.astype(BF16)
        tr[0, s, rows] = grad.T.astype(BF16)
        tr[1, s, rows] = (rect * rect).T.astype(BF16)

    def partial(lo, hi):
        rows = slice(lo, hi)

        @pl.loop(0, NZ, unroll=4)
        def _(k):
            lane = cols(k, DZ)
            g[rows, lane] = nt(pg[rows, :], w[0, lane, :]).astype(BF16)

    forward(ME)
    fcx["r"] = pass_x(cb, R, c_x["r"])
    lo, hi = blk(cb, OPP, x, 0, HALF), blk(cb, OPP, x, HALF)
    c2 = send(lo, lo, XR).send(hi, hi, XL)
    c3 = send(hi, hi, XR).send(lo, lo, XL)
    partial(ME * TB, L * TB)
    pass_y(xb, xr, x_y["r"], fxy, *MID)
    fxy2 = pass_y(xb, x2, x_y["2"])
    fcx["l"].wait()
    forward(L)
    fcx["r"].wait()
    forward(R)
    fcx["2"] = pass_x(cb, OPP, c2)
    partial(L * TB, OPP * TB)
    fxym.wait()
    mid = blk(xb, OPP, x, *MID)
    fmid = send(mid, mid, XR).send(mid, mid, XL)

    def part(slot, r, n, lane=slice(None)):
        return g.at[slot * TB + r:slot * TB + r + n, lane]

    h1b = Batch()
    h1b.send(part(R, 64, 64), rb.at[0, 64:128, :], YR)
    h1b.send(part(L, 0, 64), rb.at[1, 0:64, :], YL)
    far, right, left = cols(x2, FX), cols(xr, FX), cols(xl, FX)
    h2, h2b = {}, Batch()

    def first_x(slots):
        batch = Batch()
        for slot in slots:
            batch.send(part(slot, 128, 64, far), re.at[0, slot], XR)
            batch.send(part(slot, 192, 64, far), re.at[1, slot], XL)
            h2[slot] = batch
        return batch

    def next_x(slot):
        h2b.send(part(slot, 192, 64, right), rf.at[0, slot, 64:128], XR)
        h2b.send(part(slot, 128, 64, left), rf.at[1, slot, 0:64], XL)

    def last_x(slot):
        sf[0, slot] = (part(slot, 128, 64, right)[...].astype(F32) + re[0, slot].astype(F32)).astype(BF16)
        h2b.send(sf.at[0, slot], rf.at[0, slot, 0:64], XR)
        sf[1, slot] = (part(slot, 192, 64, left)[...].astype(F32) + re[1, slot].astype(F32)).astype(BF16)
        h2b.send(sf.at[1, slot], rf.at[1, slot, 64:128], XL)

    h2early = first_x((ME, L, R))
    for slot in (ME, L, R):
        next_x(slot)

    down = ([(0, 4), (1, 3), (0, 3), (1, 2), (0, 2), (1, 1), (0, 1)],
            [(1, 4), (0, 3), (1, 3), (0, 2), (1, 2), (0, 1), (1, 1)])
    todo = []
    for i in range(7):
        for way in range(2):
            u, k = down[way][i]
            todo.append((u, k if way == 0 else -k))
    todo += [(0, 0), (1, 0)]
    wsum = []

    def term(n, rows, lo, hi):
        u, k = todo[n]
        return nn(tr[u, rows, lo * TB:hi * TB], (xb, cb)[u][lo * TB:hi * TB, cols(step(z, k, NZ), DZ)])

    def early(*which):
        for n in which:
            gp[n] = term(n, slice(None), 0, 3)

    def give(batch, n, value):
        u, k = todo[n]
        az = step(z, k, NZ)
        gs[u, az] = value.astype(BF16)
        batch.send(gs.at[u, az], pb.at[u, az], PC)

    def keep(n, value):
        u, k = todo[n]
        gt[u, step(z, k, NZ)] = value

    def give_pair(i):
        batch = Batch()
        for n in (2 * i, 2 * i + 1):
            give(batch, n, gp[n, HB:] + term(n, slice(HB, 2 * HB), 3, 4))
        wsum.append(batch)

    def keep_pair(i):
        for n in (2 * i, 2 * i + 1):
            keep(n, gp[n, :HB] + term(n, slice(0, HB), 3, 4))

    def chunks(i):
        batch = Batch()
        for n in (2 * i, 2 * i + 1):
            value = gp[n] + term(n, slice(None), 3, 4)
            give(batch, n, value[HB:])
            keep(n, value[:HB])
        wsum.append(batch)

    early(*range(14))

    orow = slice(OPP * TB, OPP * TB + TB)
    def gather_terms(n, buf, where, first=False):
        for ax in where:
            lane = cols(ax, FX)
            more = nn(buf[orow, lane], w[n, lane, :])
            acc[n] = more if first else acc[n] + more
            first = False

    c3.wait()
    gather_terms(1, cb, (x, xl, xr), True)
    gather_terms(0, xb, (x,), True)
    fcx["2"].wait()
    gather_terms(1, cb, (x2,))
    fxy.wait()
    fmid.wait()
    gather_terms(0, xb, (xl, xr))
    fxy2.wait()
    for h in (1, 0):
        s = slice(h * HB, (h + 1) * HB)
        finish(OPP, s, acc[0, :, s] + nn(xb[orow, far], w[0, far, s]), acc[1, :, s])
        if h == 1:
            give_pair(0)

    gz = []

    away = 1 - lax.div(y, 2)
    sides = (cols(away, DZ // 2), cols(1 - away, DZ // 2))

    WHOLE, TOP, LOW = slice(None), slice(0, HB // 2), slice(HB // 2, HB)

    def total(u, k, lane, rows=WHOLE):
        az = step(z, k, NZ)
        return gt[u, az, rows, lane] + pb[u, az, rows, lane].astype(F32)

    def gsend(i, halves=(0, 1)):
        if 0 in halves:
            wsum[i].wait()
            gz.append([])
        for half in halves:
            lane = sides[half]
            if i >= 2:
                gz[i - 2][half].wait()
            for rows in (TOP, LOW) if (i, half) == (6, 1) else (WHOLE,):
                batch = Batch()
                for way in range(2):
                    u, k = down[way][i]
                    value = total(u, k if way == 0 else -k, lane, rows)
                    if i >= 2:
                        value = value + rz[way, i - 2, rows, lane].astype(F32)
                    sz[way, i, rows, lane] = value.astype(BF16)
                    ref = (way, i, rows, lane)
                    batch.send(sz.at[ref], rz.at[ref], (ZR, ZL)[way])
                gz[i].append(batch)

    keep_pair(0)
    partial(OPP * TB, OPP * TB + HALF)
    h1 = []
    for r in (0, 32):
        h1.append(send(part(OPP, r, 32), ra.at[0, r:r + 32], YR)
                  .send(part(OPP, 64 + r, 32), ra.at[1, r:r + 32], YL))
    gsend(0)
    chunks(1)
    partial(OPP * TB + HALF, OPP * TB + TB)
    first_x((OPP,))
    next_x(OPP)
    gsend(1)
    h2early.wait()
    for slot in (ME, L, R):
        last_x(slot)
    chunks(2)
    early(14, 15)
    gsend(2)
    chunks(3)
    def next_y(n, r):
        h1[n].wait()
        sb[0, r:r + 32] = (part(R, r, 32)[...].astype(F32) + ra[0, r:r + 32].astype(F32)).astype(BF16)
        h1b.send(sb.at[0, r:r + 32], rb.at[0, r:r + 32, :], YR)
        sb[1, r:r + 32] = (part(L, 64 + r, 32)[...].astype(F32) + ra[1, r:r + 32].astype(F32)).astype(BF16)
        h1b.send(sb.at[1, r:r + 32], rb.at[1, 64 + r:96 + r, :], YL)

    next_y(0, 0)
    gsend(3)
    h2[OPP].wait()
    last_x(OPP)
    next_y(1, 32)
    chunks(4)
    gsend(4)
    chunks(5)
    chunks(6)
    gsend(5, (0,))

    h2b.wait()
    here = cols(x, FX)
    for slot in range(4):
        q2[slot] = (part(slot, 128, 128, here)[...].astype(F32)
                    + rf[0, slot].astype(F32) + rf[1, slot].astype(F32))
    sh[0] = q2[OPP].astype(BF16)
    sh[1, 64:128] = q2[R, 64:128, :].astype(BF16)
    sh[2, 0:64] = q2[L, 0:64, :].astype(BF16)
    v2 = send(sh.at[0, 0:64, :], rg.at[0], YR).send(sh.at[0, 64:128, :], rg.at[1], YL)
    v2b = Batch()
    v2b.send(sh.at[1, 64:128, :], rh.at[0, 64:128, :], YR)
    v2b.send(sh.at[2, 0:64, :], rh.at[1, 0:64, :], YL)
    chunks(7)
    h1b.wait()
    for k in range(NX):
        s = slice(k * FX, (k + 1) * FX)
        q1[k] = g[0:128, s].astype(F32) + rb[0, :, s].astype(F32) + rb[1, :, s].astype(F32)
    sd[0] = q1[x2].astype(BF16)
    sd[1, 64:128] = q1[xr, 64:128, :].astype(BF16)
    sd[2, 0:64] = q1[xl, 0:64, :].astype(BF16)
    v1 = send(sd.at[0, 0:64, :], rc.at[0], XR).send(sd.at[0, 64:128, :], rc.at[1], XL)
    v1b = Batch()
    v1b.send(sd.at[1, 64:128, :], rd.at[0, 64:128, :], XR)
    v1b.send(sd.at[2, 0:64, :], rd.at[1, 0:64, :], XL)
    gsend(6, (0,))
    gsend(5, (1,))
    gsend(6, (1,))
    v2.wait()
    sh[1, 0:64] = (q2[R, 0:64, :] + rg[0].astype(F32)).astype(BF16)
    v2b.send(sh.at[1, 0:64, :], rh.at[0, 0:64, :], YR)
    sh[2, 64:128] = (q2[L, 64:128, :] + rg[1].astype(F32)).astype(BF16)
    v2b.send(sh.at[2, 64:128, :], rh.at[1, 64:128, :], YL)
    v1.wait()
    sd[1, 0:64] = (q1[xr, 0:64, :] + rc[0].astype(F32)).astype(BF16)
    v1b.send(sd.at[1, 0:64, :], rd.at[0, 0:64, :], XR)
    sd[2, 64:128] = (q1[xl, 64:128, :] + rc[1].astype(F32)).astype(BF16)
    v1b.send(sd.at[2, 64:128, :], rd.at[1, 64:128, :], XL)
    own, other = cols(c, 256), cols(o, 256)
    ends = Batch()
    def finish_rows(r, value, n):
        q1[n] = value
        fp[r:r + 128] = q1[n, :, other].astype(BF16)
        row = pl.ds(pl.multiple_of(c * TB + r, 128), 128)
        ends.send(fp.at[r:r + 128], og.at[row, :], PC)
        og[row, :] = q1[n, :, own].astype(BF16)

    scale = 1.0 / 128.0
    ops = Batch()
    wsum[7].wait()
    there = cols(y, HB)
    odd = lax.rem(y, 2)
    near = 1 - odd

    def zlast(u, lane, rows=WHOLE):
        value = total(u, 0, lane, rows)
        value = value + rz[0, 6 - u, rows, lane].astype(F32) + rz[1, 5 + u, rows, lane].astype(F32)
        return (value * scale).T.astype(BF16)

    gz[5][0].wait()
    gz[6][0].wait()
    for u in range(2):
        fs_s[u, 0] = zlast(u, sides[0])
        ops.send(fs_s.at[u, 0, cols(odd, RY), :], ow.at[u, :, there], Y2, small=True)
        ops.send(fs_s.at[u, 0, cols(near, RY), :], ow.at[u, :, there], ACROSS, small=True)
    gz[5][1].wait()
    for part_of, rows in enumerate((TOP, LOW)):
        gz[6][1 + part_of].wait()
        lane = pl.ds(pl.multiple_of(y * HB + part_of * 128, 128), 128)
        for u in range(2):
            fs_s[u, 1, :, rows] = zlast(u, sides[1], rows)
            ops.send(fs_s.at[u, 1, cols(near, RY), rows], ow.at[u, :, lane], MATE, small=True)
    for u in range(2):
        ow[u, :, there] = fs_s[u, 1, cols(odd, RY), :]

    v1b.wait()
    finish_rows(0, q1[x] + rd[0].astype(F32) + rd[1].astype(F32), 0)
    v2b.wait()
    finish_rows(128, q2[ME] + rh[0].astype(F32) + rh[1].astype(F32), 1)

    ops.wait()
    ends.wait()
    for k, (n, _) in enumerate(groups):
        ref = span(n)
        pltpu.make_async_copy(ref, ref, ssem.at[k]).wait()


def finisher(ow, og, ig_out, ug_out, dg_out, fv, sem):
    stores = [pltpu.make_async_copy(og, ig_out, sem.at[0])]
    stores[0].start()
    for u, out in ((0, ug_out), (1, dg_out)):
        fv[u] = ow[u].astype(F32)
        stores.append(pltpu.make_async_copy(fv.at[u], out, sem.at[1 + u]))
        stores[-1].start()
    for copy in stores:
        copy.wait()


def per_device(normed_input, cotangent, up_weight, down_weight):
    bf = lambda *s: pltpu.VMEM(s, BF16)
    f4 = lambda *s: pltpu.VMEM(s, F32)
    hbm = pl.BlockSpec(memory_space=pl.ANY)
    vmem = pl.BlockSpec(memory_space=pltpu.VMEM)
    shape = jax.ShapeDtypeStruct
    ow, og = pl.pallas_call(
        kernel,
        out_shape=(bf(2, RY, 4 * HB), bf(2 * TB, 256)),
        in_specs=[hbm] * 4,
        out_specs=(vmem,) * 2,
        scratch_shapes=[
            bf(NY * TB, D), bf(NY * TB, D),
            bf(2, D, 2 * HB),
            bf(TB, 256), bf(TB, 256),
            bf(2, RY, 4 * HB),
            bf(NY * TB, 2 * HB),
            bf(2, 2 * HB, NY * TB),
            f4(2, TB, 2 * HB),
            f4(2 * NZ, 2 * HB, DZ),
            f4(2, NZ, HB, DZ),
            bf(2, NZ, HB, DZ), bf(2, NZ, HB, DZ),
            bf(2, 7, HB, DZ), bf(2, 7, HB, DZ),
            bf(2, 2, DZ // 2, HB),
            bf(NY * TB, D),
            bf(2, 64, D), bf(2, 128, D), bf(2, 64, D),
            f4(NX, 128, FX),
            bf(2, 64, FX), bf(2, 128, FX), bf(3, 128, FX),
            bf(2, NY, 64, FX), bf(2, NY, 128, FX), bf(2, NY, 64, FX),
            f4(NY, 128, FX),
            bf(2, 64, FX), bf(2, 128, FX), bf(3, 128, FX),
            bf(TB, 256),
            pltpu.SemaphoreType.DMA((5,)),
            pltpu.SemaphoreType.DMA((SENDS,)),
            pltpu.SemaphoreType.DMA((RECVS,)),
        ],
        compiler_params=pltpu.CompilerParams(
            collective_id=0, has_side_effects=True, vmem_limit_bytes=60 * 1024 * 1024
        ),
    )(normed_input, cotangent, up_weight, down_weight.T)
    ig, ug, dg = pl.pallas_call(
        finisher,
        out_shape=(shape((2 * TB, 256), BF16), shape((RY, 4 * HB), F32), shape((RY, 4 * HB), F32)),
        in_specs=[vmem] * 2,
        out_specs=(hbm,) * 3,
        scratch_shapes=[f4(2, RY, 4 * HB), pltpu.SemaphoreType.DMA((3,))],
    )(*(pltpu.with_memory_space_constraint(a, pltpu.VMEM) for a in (ow, og)))
    return ig, ug, dg.T


def solution(mesh):
    return jax.shard_map(
        per_device, mesh=mesh,
        in_specs=(P("fs", "tp"), P("fs", "tp"), P("fs", "tp"), P("tp", "fs")),
        out_specs=(P("fs", "tp"), P("fs", "tp"), P("tp", "fs")),
        check_vma=False,
    )
```
